32 devices in a mesh: sp: 16 (over z, y, x), tp: 2 (over core).
Axes of the slice: x: 2, y: 2, z: 4, core: 2. Of those that a mesh axis runs over, the one named last changes fastest.
Arguments:
- prompt: bfloat16 [2, 3072, 4096], P(None, 'sp'), as said below
- w_key: bfloat16 [4096, 2048], P('sp', 'tp'), may hold values from -0.09375 to 0.09375
- w_value: bfloat16 [4096, 4096], P('sp', 'tp'), may hold values from -0.09375 to 0.09375
- w_igate: bfloat16 [4096, 8], replicated, may hold values from -0.09375 to 0.09375
- w_fgate: bfloat16 [4096, 8], replicated, may hold values from -0.09375 to 0.09375
- input_bias: float32 [8], replicated, may hold values from -1 to 120
- forget_bias: float32 [8], replicated, may hold values from 4 to 20
- new_query: bfloat16 [2, 8, 256], P(None, 'tp'), may hold values from -6 to 6
- new_key: bfloat16 [2, 8, 256], P(None, 'tp'), may hold values from -6 to 6
- new_value: bfloat16 [2, 8, 512], P(None, 'tp'), may hold values from -6 to 6
- new_gates: float32 [2, 2, 8], P(None, None, 'tp'), may hold values from 2 to 9
Outputs:
- cache_memory: bfloat16 [2, 8, 256, 512], P(None, 'tp', 'sp')
- cache_norm: float32 [2, 8, 256], P(None, 'tp', 'sp')
- cache_max: float32 [2, 8], P(None, 'tp')
- first_read: bfloat16 [2, 8, 512], P(None, 'tp')
The draws below stay inside these ranges and needn't reach their ends.
Inputs may be any that keep to these rules, and one draw needn't show every extreme that they name: `prompt`: Real-valued features, each entry drawn independently; their magnitude differs from one block of 192 positions to the next.
All inputs are finite; a program needn't handle non-finite values.
Results may differ from the reference program's by a relative error of at most 0.019.
Values may be sent and summed in bfloat16 or wider, within the bound.
A program may use at most 64 MiB of HBM per device.

```python
import math
import jax
import jax.numpy as jnp
from jax import lax

D = 4096
HEADS = 8
DK = 256
DV = 512
SEQS = 2
SPAN = 192
LEN = 3072


def draw_prompt(key, part):
    first, second = jax.random.split(jax.random.fold_in(key, 11))
    base = jax.random.normal(first, (SEQS, LEN // SPAN, SPAN, D), jnp.float32)
    lower, upper = (0.6, 1.7)
    scales = jnp.exp(jax.random.uniform(second, (SEQS, LEN // SPAN, 1, 1), jnp.float32, math.log(lower), math.log(upper)))
    return (base * scales).reshape(SEQS, LEN, D).astype(jnp.bfloat16)


def draw_input_bias(key, part):
    inner = jax.random.fold_in(key, 23)
    return jax.random.uniform(inner, (HEADS,), jnp.float32, -1.0, 1.0)


def draw_forget_bias(key, part):
    first, second, third = jax.random.split(jax.random.fold_in(key, 37), 3)
    picks = jax.random.randint(first, (HEADS,), 0, 8)
    quick = picks < 4
    slow_value = math.log(float(LEN)) + jax.random.uniform(second, (HEADS,), jnp.float32, 1.5, 2.5)
    quick_value = jax.random.uniform(third, (HEADS,), jnp.float32, 4.0, 5.0)
    return jnp.where(quick, quick_value, slow_value)


def shard_levels(own_key, dims, cuts, least, top_value):
    level = 1.0
    for position, parts in cuts:
        heights = jax.random.uniform(jax.random.fold_in(jax.random.fold_in(own_key, 6), position), (parts,), jnp.float32, least / len(cuts), top_value / len(cuts))
        level = level * jnp.repeat(jnp.exp(heights), dims[position] // parts).reshape((-1,) + (1,) * (len(dims) - 1 - position))
    return level


def normal_values(own_key, dims, deviation, limit, shards=(), held_as=jnp.bfloat16):
    result = deviation * jax.random.normal(own_key, dims, jnp.float32)
    if shards:
        result = result * shard_levels(own_key, dims, shards, -0.22, 0.18)
    return jnp.clip(result, -limit, limit).astype(held_as)


def setup_inputs(seed: int = 0) -> dict:
    key_list = jax.random.split(jax.random.key(seed), 12)
    prompt = draw_prompt(jax.random.fold_in(key_list[11], 71), 0)
    w_key = normal_values(key_list[1], (D, HEADS * DK), D ** -0.5, 0.09375, ((0, 16), (1, 2)))
    w_value = normal_values(key_list[2], (D, HEADS * DV), D ** -0.5, 0.09375, ((0, 16), (1, 2)))
    w_igate = normal_values(key_list[3], (D, HEADS), D ** -0.5, 0.09375)
    w_fgate = normal_values(key_list[4], (D, HEADS), D ** -0.5, 0.09375)
    input_bias = draw_input_bias(jax.random.fold_in(key_list[11], 71), 0)
    forget_bias = draw_forget_bias(jax.random.fold_in(key_list[11], 71), 0)
    new_query = normal_values(key_list[7], (SEQS, HEADS, DK), 1.0, 6.0, ((1, 2),))
    new_key = normal_values(key_list[8], (SEQS, HEADS, DK), 1.0, 6.0, ((1, 2),))
    new_value = normal_values(key_list[9], (SEQS, HEADS, DV), 1.0, 6.0, ((1, 2),))
    new_gates = jnp.clip(2.0 + 7.0 * jax.random.uniform(key_list[10], (2, SEQS, HEADS), jnp.float32) ** shard_levels(key_list[10], (2, SEQS, HEADS), ((2, 2),), -0.2, 0.2), 2.0, 9.0)
    return {"prompt": prompt, "w_key": w_key, "w_value": w_value, "w_igate": w_igate, "w_fgate": w_fgate, "input_bias": input_bias, "forget_bias": forget_bias, "new_query": new_query, "new_key": new_key, "new_value": new_value, "new_gates": new_gates}


def reference(prompt, w_key, w_value, w_igate, w_fgate, input_bias, forget_bias, new_query, new_key, new_value, new_gates):
    blocks = LEN // SPAN
    token_rows = prompt.reshape(SEQS * LEN, D)
    key_rows = jnp.dot(token_rows, w_key, preferred_element_type=jnp.float32).astype(jnp.bfloat16)
    value_rows = jnp.dot(token_rows, w_value, preferred_element_type=jnp.float32).astype(jnp.bfloat16)
    input_gate = jnp.dot(token_rows, w_igate, preferred_element_type=jnp.float32) + input_bias
    log_forget = jax.nn.log_sigmoid(jnp.dot(token_rows, w_fgate, preferred_element_type=jnp.float32) + forget_bias)
    input_gate = input_gate.reshape(SEQS, blocks, SPAN, HEADS)
    log_forget = log_forget.reshape(SEQS, blocks, SPAN, HEADS)
    block_total = jnp.sum(log_forget, axis=2)
    forget_after = block_total[:, :, None] - jnp.cumsum(log_forget, axis=2)
    log_weight = forget_after + input_gate
    block_max = jnp.max(log_weight, axis=2)
    later_total = jnp.flip(jnp.cumsum(jnp.flip(block_total, 1), axis=1), 1) - block_total
    block_lift = later_total + block_max
    global_max = jnp.max(block_lift, axis=1)
    factor = jnp.exp(block_lift - global_max[:, None])
    key_scale = DK ** -0.5
    key_blocks = key_rows.reshape(SEQS, blocks, SPAN, HEADS, DK).astype(jnp.float32)
    decayed = (jnp.exp(log_weight - block_max[:, :, None])[..., None] * key_scale * key_blocks).astype(jnp.bfloat16)
    value_blocks = value_rows.reshape(SEQS, blocks, SPAN, HEADS, DV)

    def accumulate(carry, inputs):
        memory, normal = carry
        block_keys, block_values, block_factor = inputs
        block_state = jnp.einsum('sthk,sthv->shkv', block_keys.astype(jnp.float32), block_values.astype(jnp.float32),
                                 precision=lax.Precision.HIGHEST)
        block_norm = jnp.sum(block_keys.astype(jnp.float32), axis=1)
        memory = memory + block_factor[:, :, None, None] * block_state
        normal = normal + block_factor[:, :, None] * block_norm
        return (memory, normal), None

    inputs = (jnp.moveaxis(decayed, 1, 0), jnp.moveaxis(value_blocks, 1, 0), jnp.moveaxis(factor, 1, 0))
    start = (jnp.zeros((SEQS, HEADS, DK, DV), jnp.float32), jnp.zeros((SEQS, HEADS, DK), jnp.float32))
    (memory, normal), _ = lax.scan(accumulate, start, inputs)
    query_full = new_query.astype(jnp.float32)
    query_state = jnp.einsum('shk,shkv->shv', query_full, memory, precision=lax.Precision.HIGHEST)
    query_norm = jnp.sum(query_full * normal, axis=-1)
    forget_new = jax.nn.log_sigmoid(new_gates[1])
    input_new = new_gates[0]
    mixed = jnp.maximum(forget_new + global_max, input_new)
    carried = jnp.exp(forget_new + global_max - mixed)
    fresh = jnp.exp(input_new - mixed)
    own_score = jnp.sum(query_full * new_key.astype(jnp.float32), axis=-1) * key_scale
    numer = carried[..., None] * query_state + (fresh * own_score)[..., None] * new_value.astype(jnp.float32)
    denom = carried * query_norm + fresh * own_score
    first_read = (numer / jnp.maximum(jnp.abs(denom), 1.0)[..., None]).astype(jnp.bfloat16)
    return memory.astype(jnp.bfloat16), normal, global_max, first_read
```

```python
import functools
import jax
import jax.numpy as jnp
from jax import lax
from jax.experimental import pallas as pl
from jax.experimental.pallas import tpu as pltpu
from jax.sharding import PartitionSpec as P

CHUNKS = 4
HIGH = lax.Precision.HIGHEST


def flip(bit, change):
    return bit + change - 2 * bit * change


def log_sigmoid(v):
    return jnp.minimum(v, 0.0) - jnp.log1p(jnp.exp(-jnp.abs(v)))


def kernel(
    prompt,
    w_key,
    w_value,
    w_gate,
    gate_bias,
    new_query,
    new_key,
    new_value,
    new_gates,
    memory_out,
    norm_out,
    max_out,
    read_out,
    xb,
    wk,
    wv,
    decay,
    vals,
    weight,
    stat,
    state,
    aux,
    rmem,
    raux,
    local_sem,
    x_send,
    x_recv,
    d_send,
    d_recv,
    wk_send,
    wk_recv,
    wv_send,
    wv_recv,
    s_send,
    s_recv,
    m_send,
    m_recv,
    a_send,
    a_recv,
):
    count = lax.axis_size("sp")
    me = lax.axis_index("sp")
    core = lax.axis_index("tp")
    seqs, span, width = prompt.shape
    depth = w_key.shape[0]
    heads = new_query.shape[1]
    dk = new_query.shape[2]
    dv = new_value.shape[2]
    total_heads = gate_bias.shape[1] // 2
    key_scale = dk ** (-0.5)
    cut = width // CHUNKS
    rows_out = dk // count
    zh, zl, y, x = me // 8, (me // 4) % 2, (me // 2) % 2, me % 2
    mine = zl * 2 + x

    def place(dh, dy, dz, dx):
        return flip(zh, dh) * 8 + flip(zl, dz) * 4 + flip(y, dy) * 2 + flip(x, dx)

    def remote(src, dst, send, recv, sp, tp):
        return pltpu.make_async_remote_copy(
            src_ref=src,
            dst_ref=dst,
            send_sem=send,
            recv_sem=recv,
            device_id=(sp, tp),
            device_id_type=pl.DeviceIdType.MESH,
        )

    ring = [(0, 0), (0, 1), (1, 0), (1, 1)]
    clique = [(0, 0), (0, 1), (1, 0), (1, 1)]
    sent = []

    def go(copy):
        copy.start()
        sent.append(copy)

    barrier = pltpu.get_barrier_semaphore()
    for off in range(1, count):
        pl.semaphore_signal(
            barrier,
            inc=1,
            device_id=((me + off) % count, core),
            device_id_type=pl.DeviceIdType.MESH,
        )
    pl.semaphore_signal(
        barrier, inc=1, device_id=(me, 1 - core), device_id_type=pl.DeviceIdType.MESH
    )

    def w_rows(slot):
        q, r = slot // 4, slot % 4
        src = place(*clique[q], *ring[r])
        return pl.ds(pl.multiple_of(src * depth, depth), depth)

    own_x = []
    for s in range(seqs):
        c = pltpu.make_async_copy(
            prompt.at[s], xb.at[0, pl.ds(s * span, span)], local_sem.at[s]
        )
        c.start()
        own_x.append(c)
    kcols = pl.ds(pl.multiple_of(mine * dk, dk), dk)
    vcols = pl.ds(pl.multiple_of(mine * dv, dv), dv)
    own_rows = w_rows(0)
    own_k = pltpu.make_async_copy(w_key.at[:, kcols], wk.at[own_rows], local_sem.at[2])
    own_v = pltpu.make_async_copy(w_value.at[:, vcols], wv.at[own_rows], local_sem.at[3])
    own_k.start()
    own_v.start()
    pl.semaphore_wait(barrier, count)

    for r in (1, 2, 3):
        dz, dx = ring[r]
        peer = place(0, 0, dz, dx)
        theirs = flip(zl, dz) * 2 + flip(x, dx)
        kc = pl.ds(pl.multiple_of(theirs * dk, dk), dk)
        vc = pl.ds(pl.multiple_of(theirs * dv, dv), dv)
        go(remote(w_key.at[:, kc], wk.at[own_rows], wk_send.at[r], wk_recv.at[r], peer, core))
        go(remote(w_value.at[:, vc], wv.at[own_rows], wv_send.at[r], wv_recv.at[r], peer, core))

    def w_relay(slot, to, tag):
        rows = w_rows(slot)
        q = slot // 4
        there = (q + to[0] * 2 + to[1]) * 4 + slot % 4
        peer = place(to[0], to[1], 0, 0)
        go(remote(wk.at[rows], wk.at[rows], wk_send.at[tag], wk_recv.at[there], peer, core))
        go(remote(wv.at[rows], wv.at[rows], wv_send.at[tag], wv_recv.at[there], peer, core))

    def w_wait(slot):
        rows = w_rows(slot)
        pltpu.make_async_copy(wk.at[rows], wk.at[rows], wk_recv.at[slot]).wait()
        pltpu.make_async_copy(wv.at[rows], wv.at[rows], wv_recv.at[slot]).wait()

    def x_part(slot, seq_rows, k):
        return xb.at[slot, seq_rows, pl.ds(k * cut, cut)]

    my_rows = pl.ds(pl.multiple_of(core * span, span), span)
    other_rows = pl.ds(pl.multiple_of((1 - core) * span, span), span)
    to_x, to_z = place(0, 0, 0, 1), place(0, 0, 1, 0)

    def x_send_own(slot, k, peer):
        go(
            remote(
                prompt.at[core, :, pl.ds(k * cut, cut)],
                x_part(slot, my_rows, k),
                x_send.at[slot, k],
                x_recv.at[slot, k],
                peer,
                core,
            )
        )

    def x_wait(slot, k):
        part = x_part(slot, my_rows, k)
        pltpu.make_async_copy(part, part, x_recv.at[slot, k]).wait()

    def x_across(slot, k):
        part = x_part(slot, my_rows, k)
        go(remote(part, part, d_send.at[slot, k], d_recv.at[slot, k], me, 1 - core))

    def d_wait(slot, k):
        part = x_part(slot, other_rows, k)
        pltpu.make_async_copy(part, part, d_recv.at[slot, k]).wait()

    x_send_own(2, 0, to_z)
    for k in range(CHUNKS):
        x_send_own(1, k, to_x)
    own_k.wait()
    own_v.wait()
    w_relay(0, (1, 0), 4)
    w_relay(0, (0, 1), 8)
    for r in (1, 2, 3):
        w_wait(r)
        w_relay(r, (1, 0), 4 + r)
        w_relay(r, (0, 1), 8 + r)
        x_send_own(2, r, to_z)
    for c in own_x:
        c.wait()

    lane = lax.broadcasted_iota(jnp.int32, (seqs * span, 2 * total_heads), 1)
    head = core * heads + mine
    at_t = lax.broadcasted_iota(jnp.int32, (span, span), 0)
    at_u = lax.broadcasted_iota(jnp.int32, (span, span), 1)
    after = (at_u > at_t).astype(jnp.float32)
    stat_row = lax.broadcasted_iota(jnp.int32, (8, 128), 0)
    stat_lane = lax.broadcasted_iota(jnp.int32, (8, 128), 1)

    def gates(r, table):
        both = jnp.dot(xb[r], w_gate[...], preferred_element_type=jnp.float32) + gate_bias[...]
        gate_in = jnp.sum(jnp.where(lane == head, both, 0.0), axis=1, keepdims=True)
        gate_f = jnp.sum(
            jnp.where(lane == total_heads + head, both, 0.0), axis=1, keepdims=True
        )
        forget = log_sigmoid(gate_f)
        for s in range(seqs):
            part = forget[s * span : (s + 1) * span]
            wide = jnp.broadcast_to(part, (span, 128))
            later = jnp.dot(after, wide, precision=HIGH, preferred_element_type=jnp.float32)
            level = later[:, 0:1] + gate_in[s * span : (s + 1) * span]
            top = jnp.max(level, axis=0, keepdims=True)
            total = jnp.sum(part, axis=0, keepdims=True)
            weight[r, s * span : (s + 1) * span] = jnp.broadcast_to(
                jnp.exp(level - top) * key_scale, (span, 128)
            )
            hit = stat_row == r * seqs + s
            table = jnp.where(hit & (stat_lane == 0), total, table)
            table = jnp.where(hit & (stat_lane == 1), top, table)
        return table

    table = gates(0, jnp.zeros((8, 128), jnp.float32))
    for k in range(CHUNKS):
        w_wait(8 + k)
        w_relay(8 + k, (0, 1), 12 + k)
        x_wait(2, k)
        go(
            remote(
                x_part(2, my_rows, k),
                x_part(3, my_rows, k),
                x_send.at[3, k],
                x_recv.at[3, k],
                to_x,
                core,
            )
        )
        x_across(2, k)
        x_wait(1, k)
        x_across(1, k)
    for k in range(CHUNKS):
        d_wait(1, k)
        d_wait(2, k)
    table = gates(1, table)
    table = gates(2, table)
    for k in range(CHUNKS):
        x_wait(3, k)
        x_across(3, k)
    for k in range(CHUNKS):
        d_wait(3, k)
    table = gates(3, table)
    stat[0] = table
    for slot in (4, 5, 6, 7, 12, 13, 14, 15):
        w_wait(slot)

    def project(r, carry):
        def step(k, acc):
            at = pl.ds(pl.multiple_of(k * cut, cut), cut)
            rows = xb[r, :, at]
            return (
                acc[0] + jnp.dot(rows, wk[at], preferred_element_type=jnp.float32),
                acc[1] + jnp.dot(rows, wv[at], preferred_element_type=jnp.float32),
            )

        keys, values = lax.fori_loop(
            0,
            CHUNKS,
            step,
            (
                jnp.zeros((seqs * span, dk), jnp.float32),
                jnp.zeros((seqs * span, dv), jnp.float32),
            ),
        )
        keys = keys.astype(jnp.bfloat16).astype(jnp.float32)
        decay[r] = (weight[r, :, 0:1] * keys).astype(jnp.bfloat16)
        vals[r] = values.astype(jnp.bfloat16)
        return carry

    project(0, 0)
    for q in (1, 2, 3):
        dh, dy = clique[q]
        go(
            remote(
                stat.at[0], stat.at[q], s_send.at[q], s_recv.at[q], place(dh, dy, 0, 0), core
            )
        )
    lax.fori_loop(1, 4, project, 0)
    for q in (1, 2, 3):
        pltpu.make_async_copy(stat.at[q], stat.at[q], s_recv.at[q]).wait()

    stats = jnp.concatenate([stat[q] for q in range(4)], axis=0)

    def spot(dim):
        n = lax.broadcasted_iota(jnp.int32, (32, 32), dim)
        dh, dy, dz, dx = n // 16, (n // 8) % 2, (n // 4) % 2, (n // 2) % 2
        where = flip(zh, dh) * 8 + flip(zl, dz) * 4 + flip(y, dy) * 2 + flip(x, dx)
        return where, n % 2

    (pos_a, seq_a), (pos_b, seq_b) = spot(0), spot(1)
    later_mask = ((pos_b > pos_a) & (seq_a == seq_b)).astype(jnp.float32)
    later = jnp.dot(later_mask, stats, precision=HIGH, preferred_element_type=jnp.float32)
    lift = later[:, 0:1] + stats[:, 1:2]
    parity = lax.broadcasted_iota(jnp.int32, (32, 1), 0) % 2
    highest = [
        jnp.max(jnp.where(parity == s, lift, -jnp.inf), axis=0, keepdims=True)
        for s in range(seqs)
    ]
    factor = jnp.exp(lift - jnp.where(parity == 0, highest[0], highest[1]))

    pick = lax.broadcasted_iota(jnp.int32, (heads, dk), 0) == mine
    ones = jnp.ones((8, span), jnp.bfloat16)
    aux_row = lax.broadcasted_iota(jnp.int32, (1, 128), 1)
    tail = jnp.zeros((1, 128), jnp.float32)
    for s in range(seqs):
        sums = jnp.zeros((dk, dv), jnp.float32)
        norms = jnp.zeros((8, dk), jnp.float32)
        for r in range(4):
            d = decay[r, s * span : (s + 1) * span]
            v = vals[r, s * span : (s + 1) * span]
            f = factor[r * seqs + s : r * seqs + s + 1, 0:1]
            sums = sums + f * lax.dot_general(
                d, v, (((0,), (0,)), ((), ())), preferred_element_type=jnp.float32
            )
            norms = norms + f * jnp.dot(ones, d, preferred_element_type=jnp.float32)
        state[s] = sums.astype(jnp.bfloat16)
        query = jnp.sum(
            jnp.where(pick, new_query[s].astype(jnp.float32), 0.0), axis=0, keepdims=True
        )
        seen = jnp.dot(
            jnp.broadcast_to(query, (8, dk)),
            sums,
            precision=HIGH,
            preferred_element_type=jnp.float32,
        )
        for k in range(dv // 128):
            aux[s * 4 + k : s * 4 + k + 1] = seen[0:1, k * 128 : (k + 1) * 128]
        for k in range(dk // 128):
            row = 8 + s * 2 + k
            aux[row : row + 1] = norms[0:1, k * 128 : (k + 1) * 128]
        dot_norm = jnp.sum(query * norms[0:1], axis=1, keepdims=True)
        tail = jnp.where(aux_row == s, highest[s], tail)
        tail = jnp.where(aux_row == 2 + s, dot_norm, tail)
    aux[12:13] = tail
    aux[13:16] = jnp.zeros((3, 128), jnp.float32)

    def cut_rows(sp):
        return pl.ds(pl.multiple_of(sp * rows_out, rows_out), rows_out)

    for off in range(1, count):
        peer = (me + off) % count
        go(
            remote(
                state.at[:, cut_rows(peer)],
                rmem.at[me],
                m_send.at[off],
                m_recv.at[off],
                peer,
                core,
            )
        )
        go(remote(aux, raux.at[me], a_send.at[off], a_recv.at[off], peer, core))
    rmem[me] = state[:, cut_rows(me), :]
    raux[me] = aux[...]

    def stack(ref):
        return jnp.concatenate([ref[s].astype(jnp.float32) for s in range(seqs)], axis=0)

    queries = stack(new_query)
    own = jnp.sum(queries * stack(new_key), axis=1, keepdims=True) * key_scale
    gate_in, gate_f = new_gates[:, 0:1], log_sigmoid(new_gates[:, 1:2])
    token_values = stack(new_value)

    for off in range(1, count):
        src = (me + count - off) % count
        pltpu.make_async_copy(rmem.at[src], rmem.at[src], m_recv.at[off]).wait()
        pltpu.make_async_copy(raux.at[src], raux.at[src], a_recv.at[off]).wait()

    read_rows, norm_rows, max_rows, dot_rows = [], [], [], []
    for s in range(seqs):
        for h in range(heads):
            srcs = [
                a * 8 + (h // 2) * 4 + b * 2 + h % 2 for a in range(2) for b in range(2)
            ]
            mem = rmem[srcs[0], s].astype(jnp.float32)
            both = raux[srcs[0]]
            for src in srcs[1:]:
                mem = mem + rmem[src, s].astype(jnp.float32)
                both = both + raux[src]
            memory_out[s, h] = mem.astype(jnp.bfloat16)
            read_rows.append(
                jnp.concatenate([both[s * 4 + k : s * 4 + k + 1] for k in range(dv // 128)], 1)
            )
            norm_rows.append(
                jnp.concatenate(
                    [both[8 + s * 2 + k : 9 + s * 2 + k] for k in range(dk // 128)], 1
                )
            )
            max_rows.append(raux[srcs[0], 12:13, s : s + 1])
            dot_rows.append(both[12:13, 2 + s : 3 + s])
    query_state = jnp.concatenate(read_rows, axis=0)
    norm_all = jnp.concatenate(norm_rows, axis=0)
    top = jnp.concatenate(max_rows, axis=0)
    query_norm = jnp.concatenate(dot_rows, axis=0)
    take = (
        lax.broadcasted_iota(jnp.int32, (dk, rows_out), 0)
        == me * rows_out + lax.broadcasted_iota(jnp.int32, (dk, rows_out), 1)
    ).astype(jnp.float32)
    norm_out[...] = jnp.dot(norm_all, take, precision=HIGH, preferred_element_type=jnp.float32)
    max_out[...] = top
    mixed = jnp.maximum(gate_f + top, gate_in)
    carried = jnp.exp(gate_f + top - mixed)
    fresh = jnp.exp(gate_in - mixed)
    numer = carried * query_state + (fresh * own) * token_values
    denom = carried * query_norm + fresh * own
    read_out[...] = (numer / jnp.maximum(jnp.abs(denom), 1.0)).astype(jnp.bfloat16)
    for copy in sent:
        copy.wait_send()


def by_head(
    prompt,
    w_key,
    w_value,
    w_igate,
    w_fgate,
    input_bias,
    forget_bias,
    new_query,
    new_key,
    new_value,
    new_gates,
):
    count = lax.axis_size("sp")
    seqs, span, width = prompt.shape
    depth = w_key.shape[0]
    heads, dk = new_query.shape[1:]
    dv = new_value.shape[2]
    rows = seqs * span
    w_gate = jnp.concatenate([w_igate, w_fgate], axis=1)
    gate_bias = jnp.concatenate([input_bias, forget_bias])[None]
    token_gates = new_gates.reshape(2, seqs * heads).T
    vmem = pl.BlockSpec(memory_space=pltpu.VMEM)
    hbm = pl.BlockSpec(memory_space=pl.ANY)
    dma = pltpu.SemaphoreType.DMA
    memory, norm, top, read = pl.pallas_call(
        kernel,
        out_shape=(
            jax.ShapeDtypeStruct((seqs, heads, dk // count, dv), jnp.bfloat16),
            jax.ShapeDtypeStruct((seqs * heads, dk // count), jnp.float32),
            jax.ShapeDtypeStruct((seqs * heads, 1), jnp.float32),
            jax.ShapeDtypeStruct((seqs * heads, dv), jnp.bfloat16),
        ),
        in_specs=[hbm, hbm, hbm] + [vmem] * 6,
        out_specs=(vmem, vmem, vmem, vmem),
        scratch_shapes=[
            pltpu.VMEM((4, rows, width), jnp.bfloat16),
            pltpu.VMEM((width, dk), jnp.bfloat16),
            pltpu.VMEM((width, dv), jnp.bfloat16),
            pltpu.VMEM((4, rows, dk), jnp.bfloat16),
            pltpu.VMEM((4, rows, dv), jnp.bfloat16),
            pltpu.VMEM((4, rows, 128), jnp.float32),
            pltpu.VMEM((4, 8, 128), jnp.float32),
            pltpu.VMEM((seqs, dk, dv), jnp.bfloat16),
            pltpu.VMEM((16, 128), jnp.float32),
            pltpu.VMEM((count, seqs, dk // count, dv), jnp.bfloat16),
            pltpu.VMEM((count, 16, 128), jnp.float32),
            dma((4,)),
            dma((4, CHUNKS)),
            dma((4, CHUNKS)),
            dma((4, CHUNKS)),
            dma((4, CHUNKS)),
            dma((16,)),
            dma((16,)),
            dma((16,)),
            dma((16,)),
            dma((4,)),
            dma((4,)),
            dma((count,)),
            dma((count,)),
            dma((count,)),
            dma((count,)),
        ],
        compiler_params=pltpu.CompilerParams(
            collective_id=0, has_side_effects=True, vmem_limit_bytes=60 * 1024 * 1024
        ),
    )(prompt, w_key, w_value, w_gate, gate_bias, new_query, new_key, new_value, token_gates)
    return (
        memory,
        norm.reshape(seqs, heads, dk // count),
        top.reshape(seqs, heads),
        read.reshape(seqs, heads, dv),
    )


def chosen(*args):
    prompt, new_query, new_value = args[0], args[7], args[9]
    heads = new_query.shape[1]
    count = lax.axis_size("sp")
    fits = (
        lax.axis_size("tp") == 2
        and heads == 4
        and count == 16
        and prompt.shape[0] == 2
        and new_query.shape[2] == 256
        and new_value.shape[2] == 512
    )
    return by_head(*args) if fits else per_device(*args)


def entering(value, axis, join, neutral):
    count, mine = (lax.axis_size(axis), lax.axis_index(axis))
    pieces = lax.all_gather(value, axis)
    pieces = pieces[::-1]
    mine = count - 1 - mine
    so_far = jnp.full_like(value, 0) + jnp.asarray(neutral, value.dtype)

    def turn(position, so_far):
        longer = join(so_far, pieces[position])
        return jnp.where(position < mine, longer, so_far)

    return lax.fori_loop(0, count - 1, turn, so_far)


def add_pair(earlier, later):
    return earlier + later


def per_device(
    prompt,
    w_key,
    w_value,
    w_igate,
    w_fgate,
    input_bias,
    forget_bias,
    new_query,
    new_key,
    new_value,
    new_gates,
):
    seq_count, span_len, model_width = prompt.shape
    local_heads = new_query.shape[1]
    key_size = new_query.shape[2]
    value_size = new_value.shape[2]
    key_scale = key_size ** (-0.5)
    token_rows = prompt.reshape(seq_count * span_len, model_width)
    whole_key, whole_value = (
        lax.all_gather(w_key, "sp", axis=0, tiled=True),
        lax.all_gather(w_value, "sp", axis=0, tiled=True),
    )
    key_rows = jnp.dot(token_rows, whole_key, preferred_element_type=jnp.float32).astype(
        jnp.bfloat16
    )
    value_rows = jnp.dot(token_rows, whole_value, preferred_element_type=jnp.float32).astype(
        jnp.bfloat16
    )
    head_start = lax.axis_index("tp") * local_heads
    input_all = jnp.dot(token_rows, w_igate, preferred_element_type=jnp.float32) + input_bias
    forget_all = jnp.dot(token_rows, w_fgate, preferred_element_type=jnp.float32) + forget_bias
    input_gate = lax.dynamic_slice_in_dim(input_all, head_start, local_heads, 1).reshape(
        seq_count, span_len, local_heads
    )
    log_forget = jax.nn.log_sigmoid(
        lax.dynamic_slice_in_dim(forget_all, head_start, local_heads, 1)
    ).reshape(seq_count, span_len, local_heads)
    block_total = jnp.sum(log_forget, axis=1)
    forget_after = block_total[:, None] - jnp.cumsum(log_forget, axis=1)
    log_weight = forget_after + input_gate
    block_max = jnp.max(log_weight, axis=1)
    key_blocks = key_rows.reshape(seq_count, span_len, local_heads, key_size).astype(jnp.float32)
    decayed = (jnp.exp(log_weight - block_max[:, None])[..., None] * key_scale * key_blocks).astype(
        jnp.bfloat16
    )
    value_blocks = value_rows.reshape(seq_count, span_len, local_heads, value_size)
    block_norm = jnp.sum(decayed.astype(jnp.float32), axis=1)
    later_total = entering(block_total, "sp", add_pair, jnp.zeros_like(block_total))
    block_lift = later_total + block_max
    global_max = lax.pmax(block_lift, "sp")
    factor = jnp.exp(block_lift - global_max)
    scaled_norm = factor[:, :, None] * block_norm
    query_full = new_query.astype(jnp.float32)
    block_state = jnp.einsum(
        "sthk,sthv->shkv", decayed, value_blocks, preferred_element_type=jnp.float32
    )
    scaled_state = factor[:, :, None, None] * block_state
    memory_rows, norm_rows = (
        lax.psum_scatter(scaled_state, "sp", scatter_dimension=2, tiled=True),
        lax.psum_scatter(scaled_norm, "sp", scatter_dimension=2, tiled=True),
    )
    token_score = jnp.einsum(
        "shk,sthk->sth", new_query, decayed, preferred_element_type=jnp.float32
    )
    score_high = token_score.astype(jnp.bfloat16)
    score_low = (token_score - score_high.astype(jnp.float32)).astype(jnp.bfloat16)
    weighted = jnp.einsum(
        "sth,sthv->shv", score_high, value_blocks, preferred_element_type=jnp.float32
    )
    weighted = weighted + jnp.einsum(
        "sth,sthv->shv", score_low, value_blocks, preferred_element_type=jnp.float32
    )
    partial_state = factor[..., None] * weighted
    partial_norm = jnp.sum(query_full * scaled_norm, axis=-1)
    query_state, query_norm = lax.psum((partial_state, partial_norm), "sp")
    forget_new = jax.nn.log_sigmoid(new_gates[1])
    input_new = new_gates[0]
    mixed = jnp.maximum(forget_new + global_max, input_new)
    carried = jnp.exp(forget_new + global_max - mixed)
    fresh = jnp.exp(input_new - mixed)
    own_score = jnp.sum(query_full * new_key.astype(jnp.float32), axis=-1) * key_scale
    numer = carried[..., None] * query_state + (fresh * own_score)[..., None] * new_value.astype(
        jnp.float32
    )
    denom = carried * query_norm + fresh * own_score
    first_read = (numer / jnp.maximum(jnp.abs(denom), 1.0)[..., None]).astype(jnp.bfloat16)
    return (memory_rows.astype(jnp.bfloat16), norm_rows, global_max, first_read)


def solution(mesh):
    placed = (
        P(None, "sp", None),
        P("sp", "tp"),
        P("sp", "tp"),
        P(),
        P(),
        P(),
        P(),
        P(None, "tp", None),
        P(None, "tp", None),
        P(None, "tp", None),
        P(None, None, "tp"),
    )
    return jax.shard_map(
        chosen,
        mesh=mesh,
        in_specs=placed,
        out_specs=(
            P(None, "tp", "sp", None),
            P(None, "tp", "sp"),
            P(None, "tp"),
            P(None, "tp", None),
        ),
        check_vma=False,
    )
```

```python
import functools
import jax
import jax.numpy as jnp
from jax import lax
from jax.experimental import pallas as pl
from jax.experimental.pallas import tpu as pltpu
from jax.sharding import PartitionSpec as P

CHUNKS = 8
PER = CHUNKS // 4
HIGH = lax.Precision.HIGHEST


def flip(bit, change):
    return bit + change - 2 * bit * change


def log_sigmoid(v):
    return jnp.minimum(v, 0.0) - jnp.log1p(jnp.exp(-jnp.abs(v)))


def kernel(
    prompt,
    w_key,
    w_value,
    w_igate,
    w_fgate,
    input_bias,
    forget_bias,
    new_query,
    new_key,
    new_value,
    new_gates,
    memory_out,
    norm_out,
    max_out,
    read_out,
    xb,
    wk,
    wv,
    w_gate,
    key_acc,
    value_acc,
    decay,
    vals,
    weight,
    stat,
    state,
    aux,
    rmem,
    raux,
    local_sem,
    x_send,
    x_recv,
    d_send,
    d_recv,
    wk_send,
    wk_recv,
    wv_send,
    wv_recv,
    s_send,
    s_recv,
    m_send,
    m_recv,
    a_send,
    a_recv,
):
    count = lax.axis_size("sp")
    me = lax.axis_index("sp")
    core = lax.axis_index("tp")
    seqs, span, width = prompt.shape
    depth = w_key.shape[0]
    heads = new_query.shape[1]
    dk = new_query.shape[2]
    dv = new_value.shape[2]
    total_heads = input_bias.shape[1]
    key_scale = dk ** (-0.5)
    cut = width // CHUNKS
    rows_out = dk // count
    zh, zl, y, x = me // 8, (me // 4) % 2, (me // 2) % 2, me % 2
    mine = zl * 2 + x

    def place(dh, dy, dz, dx):
        return flip(zh, dh) * 8 + flip(zl, dz) * 4 + flip(y, dy) * 2 + flip(x, dx)

    def remote(src, dst, send, recv, sp, tp):
        return pltpu.make_async_remote_copy(
            src_ref=src,
            dst_ref=dst,
            send_sem=send,
            recv_sem=recv,
            device_id=(sp, tp),
            device_id_type=pl.DeviceIdType.MESH,
        )

    ring = [(0, 0), (0, 1), (1, 0), (1, 1)]
    clique = [(0, 0), (0, 1), (1, 0), (1, 1)]
    sent = []

    def go(copy):
        copy.start()
        sent.append(copy)

    barrier = pltpu.get_barrier_semaphore()
    for off in range(1, count):
        pl.semaphore_signal(
            barrier,
            inc=1,
            device_id=((me + off) % count, core),
            device_id_type=pl.DeviceIdType.MESH,
        )
    pl.semaphore_signal(
        barrier, inc=1, device_id=(me, 1 - core), device_id_type=pl.DeviceIdType.MESH
    )

    def w_rows(slot):
        q, r = slot // 4, slot % 4
        src = place(*clique[q], *ring[r])
        return pl.ds(pl.multiple_of(src * depth, depth), depth)

    own_x = []
    for s in range(seqs):
        c = pltpu.make_async_copy(
            prompt.at[s], xb.at[0, pl.ds(s * span, span)], local_sem.at[s]
        )
        c.start()
        own_x.append(c)
    kcols = pl.ds(pl.multiple_of(mine * dk, dk), dk)
    vcols = pl.ds(pl.multiple_of(mine * dv, dv), dv)
    own_rows = w_rows(0)
    own_k = pltpu.make_async_copy(w_key.at[:, kcols], wk.at[own_rows], local_sem.at[2])
    own_v = pltpu.make_async_copy(w_value.at[:, vcols], wv.at[own_rows], local_sem.at[3])
    own_k.start()
    own_v.start()
    pl.semaphore_wait(barrier, count)

    for r in (1, 2, 3):
        dz, dx = ring[r]
        peer = place(0, 0, dz, dx)
        theirs = flip(zl, dz) * 2 + flip(x, dx)
        kc = pl.ds(pl.multiple_of(theirs * dk, dk), dk)
        vc = pl.ds(pl.multiple_of(theirs * dv, dv), dv)
        go(remote(w_key.at[:, kc], wk.at[own_rows], wk_send.at[r], wk_recv.at[r], peer, core))
        go(remote(w_value.at[:, vc], wv.at[own_rows], wv_send.at[r], wv_recv.at[r], peer, core))

    def w_relay(slot, to, tag):
        rows = w_rows(slot)
        q = slot // 4
        there = (q + to[0] * 2 + to[1]) * 4 + slot % 4
        peer = place(to[0], to[1], 0, 0)
        go(remote(wk.at[rows], wk.at[rows], wk_send.at[tag], wk_recv.at[there], peer, core))
        go(remote(wv.at[rows], wv.at[rows], wv_send.at[tag], wv_recv.at[there], peer, core))

    def w_wait(slot):
        rows = w_rows(slot)
        pltpu.make_async_copy(wk.at[rows], wk.at[rows], wk_recv.at[slot]).wait()
        pltpu.make_async_copy(wv.at[rows], wv.at[rows], wv_recv.at[slot]).wait()

    def x_part(slot, seq_rows, k):
        return xb.at[slot, seq_rows, pl.ds(k * cut, cut)]

    my_rows = pl.ds(pl.multiple_of(core * span, span), span)
    other_rows = pl.ds(pl.multiple_of((1 - core) * span, span), span)
    to_x, to_z = place(0, 0, 0, 1), place(0, 0, 1, 0)

    def x_send_own(slot, k, peer):
        go(
            remote(
                prompt.at[core, :, pl.ds(k * cut, cut)],
                x_part(slot, my_rows, k),
                x_send.at[slot, k],
                x_recv.at[slot, k],
                peer,
                core,
            )
        )

    def x_wait(slot, k):
        part = x_part(slot, my_rows, k)
        pltpu.make_async_copy(part, part, x_recv.at[slot, k]).wait()

    def x_across(slot, k):
        part = x_part(slot, my_rows, k)
        go(remote(part, part, d_send.at[slot, k], d_recv.at[slot, k], me, 1 - core))

    def d_wait(slot, k):
        part = x_part(slot, other_rows, k)
        pltpu.make_async_copy(part, part, d_recv.at[slot, k]).wait()

    for k in range(PER):
        x_send_own(2, k, to_z)
    for k in range(CHUNKS):
        x_send_own(1, k, to_x)
    own_k.wait()
    own_v.wait()
    w_relay(0, (1, 0), 4)
    w_relay(0, (0, 1), 8)
    for r in (1, 2, 3):
        w_wait(r)
        w_relay(r, (1, 0), 4 + r)
        w_relay(r, (0, 1), 8 + r)
        for k in range(PER):
            x_send_own(2, r * PER + k, to_z)
    for c in own_x:
        c.wait()

    lane = lax.broadcasted_iota(jnp.int32, (seqs * span, 2 * total_heads), 1)
    head = core * heads + mine
    w_gate[...] = jnp.concatenate([w_igate[...], w_fgate[...]], axis=0)
    head_lane = lax.broadcasted_iota(jnp.int32, (1, total_heads), 1) == head
    bias_in = jnp.sum(jnp.where(head_lane, input_bias[...], 0.0), axis=1, keepdims=True)
    bias_f = jnp.sum(jnp.where(head_lane, forget_bias[...], 0.0), axis=1, keepdims=True)
    at_t = lax.broadcasted_iota(jnp.int32, (span, span), 0)
    at_u = lax.broadcasted_iota(jnp.int32, (span, span), 1)
    after = (at_u > at_t).astype(jnp.float32)
    stat_row = lax.broadcasted_iota(jnp.int32, (8, 128), 0)
    stat_lane = lax.broadcasted_iota(jnp.int32, (8, 128), 1)

    def gates(r, table):
        both = lax.dot_general(
            xb[r],
            w_gate[...],
            (((1,), (1,)), ((), ())),
            preferred_element_type=jnp.float32,
        )
        gate_in = bias_in + jnp.sum(jnp.where(lane == head, both, 0.0), axis=1, keepdims=True)
        gate_f = bias_f + jnp.sum(
            jnp.where(lane == total_heads + head, both, 0.0), axis=1, keepdims=True
        )
        forget = log_sigmoid(gate_f)
        for s in range(seqs):
            part = forget[s * span : (s + 1) * span]
            wide = jnp.broadcast_to(part, (span, 128))
            later = jnp.dot(after, wide, precision=HIGH, preferred_element_type=jnp.float32)
            level = later[:, 0:1] + gate_in[s * span : (s + 1) * span]
            top = jnp.max(level, axis=0, keepdims=True)
            total = jnp.sum(part, axis=0, keepdims=True)
            weight[r, s * span : (s + 1) * span] = jnp.broadcast_to(
                jnp.exp(level - top) * key_scale, (span, 128)
            )
            hit = stat_row == r * seqs + s
            table = jnp.where(hit & (stat_lane == 0), total, table)
            table = jnp.where(hit & (stat_lane == 1), top, table)
        return table

    def project(r, slots, first):
        def step(i, carry):
            keys = values = None
            for off in range(2):
                rows = slots(2 * i + off)
                tokens = xb[r, :, rows]
                k_part = jnp.dot(tokens, wk[rows], preferred_element_type=jnp.float32)
                v_part = jnp.dot(tokens, wv[rows], preferred_element_type=jnp.float32)
                keys = k_part if keys is None else keys + k_part
                values = v_part if values is None else values + v_part
            key_acc[r] += keys
            value_acc[r] += values
            return carry

        if first:
            key_acc[r] = jnp.zeros((seqs * span, dk), jnp.float32)
            value_acc[r] = jnp.zeros((seqs * span, dv), jnp.float32)
        return step

    def source_rows(q):
        def rows(r):
            dh, dy = clique[q]
            dz, dx = r // 2, r % 2
            src = place(dh, dy, dz, dx)
            return pl.ds(pl.multiple_of(src * depth, depth), depth)

        return rows

    def group(r, q, first=False):
        lax.fori_loop(0, 2, project(r, source_rows(q), first), 0)

    def finish(r):
        keys = key_acc[r].astype(jnp.bfloat16).astype(jnp.float32)
        decay[r] = (weight[r, :, 0:1] * keys).astype(jnp.bfloat16)
        vals[r] = value_acc[r].astype(jnp.bfloat16)

    table = gates(0, jnp.zeros((8, 128), jnp.float32))
    group(0, 0, True)
    for k in range(4):
        w_wait(8 + k)
        w_relay(8 + k, (0, 1), 12 + k)
        for c in range(k * PER, (k + 1) * PER):
            x_wait(2, c)
            go(
                remote(
                    x_part(2, my_rows, c),
                    x_part(3, my_rows, c),
                    x_send.at[3, c],
                    x_recv.at[3, c],
                    to_x,
                    core,
                )
            )
            x_across(2, c)
            x_wait(1, c)
            x_across(1, c)
    group(0, 2)
    for slot in range(4, 8):
        w_wait(slot)
    group(0, 1)
    for c in range(CHUNKS):
        d_wait(1, c)
    table = gates(1, table)
    for q in range(3):
        group(1, q, q == 0)
    for c in range(CHUNKS // 2):
        x_wait(3, c)
        x_across(3, c)
    for c in range(CHUNKS):
        d_wait(2, c)
    table = gates(2, table)
    for q in range(3):
        group(2, q, q == 0)
    for c in range(CHUNKS // 2, CHUNKS):
        x_wait(3, c)
        x_across(3, c)
    for slot in range(12, 16):
        w_wait(slot)
    for c in range(CHUNKS):
        d_wait(3, c)
    table = gates(3, table)
    stat[0] = table
    for r in range(3):
        group(r, 3)
        finish(r)
    for q in (1, 2, 3):
        dh, dy = clique[q]
        go(
            remote(
                stat.at[0], stat.at[q], s_send.at[q], s_recv.at[q], place(dh, dy, 0, 0), core
            )
        )
    for q in range(4):
        group(3, q, q == 0)
    finish(3)
    for q in (1, 2, 3):
        pltpu.make_async_copy(stat.at[q], stat.at[q], s_recv.at[q]).wait()

    stats = jnp.concatenate([stat[q] for q in range(4)], axis=0)

    def spot(dim):
        n = lax.broadcasted_iota(jnp.int32, (32, 32), dim)
        dh, dy, dz, dx = n // 16, (n // 8) % 2, (n // 4) % 2, (n // 2) % 2
        where = flip(zh, dh) * 8 + flip(zl, dz) * 4 + flip(y, dy) * 2 + flip(x, dx)
        return where, n % 2

    (pos_a, seq_a), (pos_b, seq_b) = spot(0), spot(1)
    later_mask = ((pos_b > pos_a) & (seq_a == seq_b)).astype(jnp.float32)
    later = jnp.dot(later_mask, stats, precision=HIGH, preferred_element_type=jnp.float32)
    lift = later[:, 0:1] + stats[:, 1:2]
    parity = lax.broadcasted_iota(jnp.int32, (32, 1), 0) % 2
    highest = [
        jnp.max(jnp.where(parity == s, lift, -jnp.inf), axis=0, keepdims=True)
        for s in range(seqs)
    ]
    factor = jnp.exp(lift - jnp.where(parity == 0, highest[0], highest[1]))

    pick = lax.broadcasted_iota(jnp.int32, (heads, dk), 0) == mine
    ones = jnp.ones((8, span), jnp.bfloat16)
    aux_row = lax.broadcasted_iota(jnp.int32, (1, 128), 1)
    tail = jnp.zeros((1, 128), jnp.float32)

    def cut_rows(sp):
        return pl.ds(pl.multiple_of(sp * rows_out, rows_out), rows_out)

    for s in range(seqs):
        sums = jnp.zeros((dk, dv), jnp.float32)
        norms = jnp.zeros((8, dk), jnp.float32)
        for r in range(4):
            d = decay[r, s * span : (s + 1) * span]
            v = vals[r, s * span : (s + 1) * span]
            f = factor[r * seqs + s : r * seqs + s + 1, 0:1]
            sums = sums + f * lax.dot_general(
                d, v, (((0,), (0,)), ((), ())), preferred_element_type=jnp.float32
            )
            norms = norms + f * jnp.dot(ones, d, preferred_element_type=jnp.float32)
        state[s] = sums.astype(jnp.bfloat16)
        query = jnp.sum(
            jnp.where(pick, new_query[s].astype(jnp.float32), 0.0), axis=0, keepdims=True
        )
        seen = jnp.dot(
            jnp.broadcast_to(query, (8, dk)),
            sums,
            precision=HIGH,
            preferred_element_type=jnp.float32,
        )
        for k in range(dv // 128):
            aux[s * 4 + k : s * 4 + k + 1] = seen[0:1, k * 128 : (k + 1) * 128]
        for k in range(dk // 128):
            row = 8 + s * 2 + k
            aux[row : row + 1] = norms[0:1, k * 128 : (k + 1) * 128]
        dot_norm = jnp.sum(query * norms[0:1], axis=1, keepdims=True)
        tail = jnp.where(aux_row == s, highest[s], tail)
        tail = jnp.where(aux_row == 2 + s, dot_norm, tail)
        for off in range(1, count):
            peer = (me + off) % count
            go(
                remote(
                    state.at[s, cut_rows(peer)],
                    rmem.at[me, s],
                    m_send.at[s, off],
                    m_recv.at[s, off],
                    peer,
                    core,
                )
            )
    aux[12:13] = tail
    aux[13:16] = jnp.zeros((3, 128), jnp.float32)
    for off in range(1, count):
        peer = (me + off) % count
        go(remote(aux, raux.at[me], a_send.at[off], a_recv.at[off], peer, core))
    rmem[me] = state[:, cut_rows(me), :]
    raux[me] = aux[...]

    def stack(ref):
        return jnp.concatenate([ref[s].astype(jnp.float32) for s in range(seqs)], axis=0)

    queries = stack(new_query)
    own = jnp.sum(queries * stack(new_key), axis=1, keepdims=True) * key_scale
    own_head = (
        lax.broadcasted_iota(jnp.int32, (seqs * heads, heads), 0) % heads
        == lax.broadcasted_iota(jnp.int32, (seqs * heads, heads), 1)
    )

    def upright(block):
        wide = jnp.concatenate(
            [jnp.broadcast_to(block[s : s + 1], (heads, heads)) for s in range(seqs)], axis=0
        )
        return jnp.sum(jnp.where(own_head, wide, 0.0), axis=1, keepdims=True)

    gate_in, gate_f = upright(new_gates[0]), log_sigmoid(upright(new_gates[1]))
    token_values = stack(new_value)

    for off in range(1, count):
        src = (me + count - off) % count
        for s in range(seqs):
            part = rmem.at[src, s]
            pltpu.make_async_copy(part, part, m_recv.at[s, off]).wait()
        pltpu.make_async_copy(raux.at[src], raux.at[src], a_recv.at[off]).wait()

    read_rows, norm_rows, max_rows, dot_rows = [], [], [], []
    for s in range(seqs):
        for h in range(heads):
            srcs = [
                a * 8 + (h // 2) * 4 + b * 2 + h % 2 for a in range(2) for b in range(2)
            ]
            mem = rmem[srcs[0], s].astype(jnp.float32)
            both = raux[srcs[0]]
            for src in srcs[1:]:
                mem = mem + rmem[src, s].astype(jnp.float32)
                both = both + raux[src]
            memory_out[s, h] = mem.astype(jnp.bfloat16)
            read_rows.append(
                jnp.concatenate([both[s * 4 + k : s * 4 + k + 1] for k in range(dv // 128)], 1)
            )
            norm_rows.append(
                jnp.concatenate(
                    [both[8 + s * 2 + k : 9 + s * 2 + k] for k in range(dk // 128)], 1
                )
            )
            max_rows.append(raux[srcs[0], 12:13, s : s + 1])
            dot_rows.append(both[12:13, 2 + s : 3 + s])
    query_state = jnp.concatenate(read_rows, axis=0)
    norm_all = jnp.concatenate(norm_rows, axis=0)
    top = jnp.concatenate(max_rows, axis=0)
    query_norm = jnp.concatenate(dot_rows, axis=0)
    take = (
        lax.broadcasted_iota(jnp.int32, (dk, rows_out), 0)
        == me * rows_out + lax.broadcasted_iota(jnp.int32, (dk, rows_out), 1)
    ).astype(jnp.float32)
    norm_out[...] = jnp.dot(norm_all, take, precision=HIGH, preferred_element_type=jnp.float32)
    max_out[...] = top
    mixed = jnp.maximum(gate_f + top, gate_in)
    carried = jnp.exp(gate_f + top - mixed)
    fresh = jnp.exp(gate_in - mixed)
    numer = carried * query_state + (fresh * own) * token_values
    denom = carried * query_norm + fresh * own
    read_out[...] = (numer / jnp.maximum(jnp.abs(denom), 1.0)).astype(jnp.bfloat16)
    for copy in sent:
        copy.wait_send()


def hand_on(memory, norm, top, read, memory_out, norm_out, max_out, read_out):
    seqs, heads = max_out.shape
    memory_out[...] = memory[...]
    at = lax.broadcasted_iota(jnp.int32, (seqs * heads, heads), 0)
    to = lax.broadcasted_iota(jnp.int32, (seqs * heads, heads), 1)
    wide = read[...].astype(jnp.float32)
    for s in range(seqs):
        rows = slice(s * heads, (s + 1) * heads)
        norm_out[s] = norm[rows]
        read_out[s] = wide[rows].astype(jnp.bfloat16)
        max_out[s : s + 1] = jnp.sum(
            jnp.where(at == s * heads + to, top[...], 0.0), axis=0, keepdims=True
        )


def by_head(
    prompt,
    w_key,
    w_value,
    w_igate,
    w_fgate,
    input_bias,
    forget_bias,
    new_query,
    new_key,
    new_value,
    new_gates,
):
    count = lax.axis_size("sp")
    seqs, span, width = prompt.shape
    depth = w_key.shape[0]
    heads, dk = new_query.shape[1:]
    dv = new_value.shape[2]
    rows = seqs * span
    vmem = pl.BlockSpec(memory_space=pltpu.VMEM)
    hbm = pl.BlockSpec(memory_space=pl.ANY)
    dma = pltpu.SemaphoreType.DMA
    memory, norm, top, read = pl.pallas_call(
        kernel,
        out_shape=(
            jax.ShapeDtypeStruct((seqs, heads, dk // count, dv), jnp.bfloat16),
            jax.ShapeDtypeStruct((seqs * heads, dk // count), jnp.float32),
            jax.ShapeDtypeStruct((seqs * heads, 1), jnp.float32),
            jax.ShapeDtypeStruct((seqs * heads, dv), jnp.bfloat16),
        ),
        in_specs=[hbm, hbm, hbm] + [vmem] * 8,
        out_specs=(vmem, vmem, vmem, vmem),
        scratch_shapes=[
            pltpu.VMEM((4, rows, width), jnp.bfloat16),
            pltpu.VMEM((width, dk), jnp.bfloat16),
            pltpu.VMEM((width, dv), jnp.bfloat16),
            pltpu.VMEM((2 * w_igate.shape[1], width), jnp.bfloat16),
            pltpu.VMEM((4, rows, dk), jnp.float32),
            pltpu.VMEM((4, rows, dv), jnp.float32),
            pltpu.VMEM((4, rows, dk), jnp.bfloat16),
            pltpu.VMEM((4, rows, dv), jnp.bfloat16),
            pltpu.VMEM((4, rows, 128), jnp.float32),
            pltpu.VMEM((4, 8, 128), jnp.float32),
            pltpu.VMEM((seqs, dk, dv), jnp.bfloat16),
            pltpu.VMEM((16, 128), jnp.float32),
            pltpu.VMEM((count, seqs, dk // count, dv), jnp.bfloat16),
            pltpu.VMEM((count, 16, 128), jnp.float32),
            dma((4,)),
            dma((4, CHUNKS)),
            dma((4, CHUNKS)),
            dma((4, CHUNKS)),
            dma((4, CHUNKS)),
            dma((16,)),
            dma((16,)),
            dma((16,)),
            dma((16,)),
            dma((4,)),
            dma((4,)),
            dma((seqs, count)),
            dma((seqs, count)),
            dma((count,)),
            dma((count,)),
        ],
        compiler_params=pltpu.CompilerParams(
            collective_id=0, has_side_effects=True, vmem_limit_bytes=60 * 1024 * 1024
        ),
    )(
        prompt,
        w_key,
        w_value,
        w_igate.T,
        w_fgate.T,
        input_bias[None],
        forget_bias[None],
        new_query,
        new_key,
        new_value,
        new_gates,
    )
    return pl.pallas_call(
        hand_on,
        out_shape=(
            jax.ShapeDtypeStruct((seqs, heads, dk // count, dv), jnp.bfloat16),
            jax.ShapeDtypeStruct((seqs, heads, dk // count), jnp.float32),
            jax.ShapeDtypeStruct((seqs, heads), jnp.float32),
            jax.ShapeDtypeStruct((seqs, heads, dv), jnp.bfloat16),
        ),
        in_specs=[vmem] * 4,
        out_specs=(vmem,) * 4,
    )(memory, norm, top, read)


def chosen(*args):
    prompt, new_query, new_value = args[0], args[7], args[9]
    heads = new_query.shape[1]
    count = lax.axis_size("sp")
    fits = (
        lax.axis_size("tp") == 2
        and heads == 4
        and count == 16
        and prompt.shape[0] == 2
        and new_query.shape[2] == 256
        and new_value.shape[2] == 512
    )
    return by_head(*args) if fits else per_device(*args)


def entering(value, axis, join, neutral):
    count, mine = (lax.axis_size(axis), lax.axis_index(axis))
    pieces = lax.all_gather(value, axis)
    pieces = pieces[::-1]
    mine = count - 1 - mine
    so_far = jnp.full_like(value, 0) + jnp.asarray(neutral, value.dtype)

    def turn(position, so_far):
        longer = join(so_far, pieces[position])
        return jnp.where(position < mine, longer, so_far)

    return lax.fori_loop(0, count - 1, turn, so_far)


def add_pair(earlier, later):
    return earlier + later


def per_device(
    prompt,
    w_key,
    w_value,
    w_igate,
    w_fgate,
    input_bias,
    forget_bias,
    new_query,
    new_key,
    new_value,
    new_gates,
):
    seq_count, span_len, model_width = prompt.shape
    local_heads = new_query.shape[1]
    key_size = new_query.shape[2]
    value_size = new_value.shape[2]
    key_scale = key_size ** (-0.5)
    token_rows = prompt.reshape(seq_count * span_len, model_width)
    whole_key, whole_value = (
        lax.all_gather(w_key, "sp", axis=0, tiled=True),
        lax.all_gather(w_value, "sp", axis=0, tiled=True),
    )
    key_rows = jnp.dot(token_rows, whole_key, preferred_element_type=jnp.float32).astype(
        jnp.bfloat16
    )
    value_rows = jnp.dot(token_rows, whole_value, preferred_element_type=jnp.float32).astype(
        jnp.bfloat16
    )
    head_start = lax.axis_index("tp") * local_heads
    input_all = jnp.dot(token_rows, w_igate, preferred_element_type=jnp.float32) + input_bias
    forget_all = jnp.dot(token_rows, w_fgate, preferred_element_type=jnp.float32) + forget_bias
    input_gate = lax.dynamic_slice_in_dim(input_all, head_start, local_heads, 1).reshape(
        seq_count, span_len, local_heads
    )
    log_forget = jax.nn.log_sigmoid(
        lax.dynamic_slice_in_dim(forget_all, head_start, local_heads, 1)
    ).reshape(seq_count, span_len, local_heads)
    block_total = jnp.sum(log_forget, axis=1)
    forget_after = block_total[:, None] - jnp.cumsum(log_forget, axis=1)
    log_weight = forget_after + input_gate
    block_max = jnp.max(log_weight, axis=1)
    key_blocks = key_rows.reshape(seq_count, span_len, local_heads, key_size).astype(jnp.float32)
    decayed = (jnp.exp(log_weight - block_max[:, None])[..., None] * key_scale * key_blocks).astype(
        jnp.bfloat16
    )
    value_blocks = value_rows.reshape(seq_count, span_len, local_heads, value_size)
    block_norm = jnp.sum(decayed.astype(jnp.float32), axis=1)
    later_total = entering(block_total, "sp", add_pair, jnp.zeros_like(block_total))
    block_lift = later_total + block_max
    global_max = lax.pmax(block_lift, "sp")
    factor = jnp.exp(block_lift - global_max)
    scaled_norm = factor[:, :, None] * block_norm
    query_full = new_query.astype(jnp.float32)
    block_state = jnp.einsum(
        "sthk,sthv->shkv", decayed, value_blocks, preferred_element_type=jnp.float32
    )
    scaled_state = factor[:, :, None, None] * block_state
    memory_rows, norm_rows = (
        lax.psum_scatter(scaled_state, "sp", scatter_dimension=2, tiled=True),
        lax.psum_scatter(scaled_norm, "sp", scatter_dimension=2, tiled=True),
    )
    token_score = jnp.einsum(
        "shk,sthk->sth", new_query, decayed, preferred_element_type=jnp.float32
    )
    score_high = token_score.astype(jnp.bfloat16)
    score_low = (token_score - score_high.astype(jnp.float32)).astype(jnp.bfloat16)
    weighted = jnp.einsum(
        "sth,sthv->shv", score_high, value_blocks, preferred_element_type=jnp.float32
    )
    weighted = weighted + jnp.einsum(
        "sth,sthv->shv", score_low, value_blocks, preferred_element_type=jnp.float32
    )
    partial_state = factor[..., None] * weighted
    partial_norm = jnp.sum(query_full * scaled_norm, axis=-1)
    query_state, query_norm = lax.psum((partial_state, partial_norm), "sp")
    forget_new = jax.nn.log_sigmoid(new_gates[1])
    input_new = new_gates[0]
    mixed = jnp.maximum(forget_new + global_max, input_new)
    carried = jnp.exp(forget_new + global_max - mixed)
    fresh = jnp.exp(input_new - mixed)
    own_score = jnp.sum(query_full * new_key.astype(jnp.float32), axis=-1) * key_scale
    numer = carried[..., None] * query_state + (fresh * own_score)[..., None] * new_value.astype(
        jnp.float32
    )
    denom = carried * query_norm + fresh * own_score
    first_read = (numer / jnp.maximum(jnp.abs(denom), 1.0)[..., None]).astype(jnp.bfloat16)
    return (memory_rows.astype(jnp.bfloat16), norm_rows, global_max, first_read)


def solution(mesh):
    placed = (
        P(None, "sp", None),
        P("sp", "tp"),
        P("sp", "tp"),
        P(),
        P(),
        P(),
        P(),
        P(None, "tp", None),
        P(None, "tp", None),
        P(None, "tp", None),
        P(None, None, "tp"),
    )
    return jax.shard_map(
        chosen,
        mesh=mesh,
        in_specs=placed,
        out_specs=(
            P(None, "tp", "sp", None),
            P(None, "tp", "sp"),
            P(None, "tp"),
            P(None, "tp", None),
        ),
        check_vma=False,
    )
```

```python
import functools
import jax
import jax.numpy as jnp
from jax import lax
from jax.experimental import pallas as pl
from jax.experimental.pallas import tpu as pltpu
from jax.sharding import PartitionSpec as P

CHUNKS = 8
PER = CHUNKS // 4
HIGH = lax.Precision.HIGHEST


def flip(bit, change):
    return bit + change - 2 * bit * change


def log_sigmoid(v):
    return jnp.minimum(v, 0.0) - jnp.log1p(jnp.exp(-jnp.abs(v)))


def kernel(
    prompt,
    w_key,
    w_value,
    w_igate,
    w_fgate,
    input_bias,
    forget_bias,
    new_query,
    new_key,
    new_value,
    new_gates,
    memory_out,
    norm_out,
    max_out,
    read_out,
    xb,
    wk,
    wv,
    w_gate,
    key_acc,
    value_acc,
    decay,
    vals,
    weight,
    stat,
    state,
    aux,
    rmem,
    raux,
    local_sem,
    x_send,
    x_recv,
    d_send,
    d_recv,
    wk_send,
    wk_recv,
    wv_send,
    wv_recv,
    s_send,
    s_recv,
    m_send,
    m_recv,
    a_send,
    a_recv,
):
    count = lax.axis_size("sp")
    me = lax.axis_index("sp")
    core = lax.axis_index("tp")
    seqs, span, width = prompt.shape
    depth = w_key.shape[0]
    heads = new_query.shape[1]
    dk = new_query.shape[2]
    dv = new_value.shape[2]
    total_heads = input_bias.shape[1]
    key_scale = dk ** (-0.5)
    cut = width // CHUNKS
    rows_out = dk // count
    zh, zl, y, x = me // 8, (me // 4) % 2, (me // 2) % 2, me % 2
    mine = zl * 2 + x

    def place(dh, dy, dz, dx):
        return flip(zh, dh) * 8 + flip(zl, dz) * 4 + flip(y, dy) * 2 + flip(x, dx)

    def remote(src, dst, send, recv, sp, tp):
        return pltpu.make_async_remote_copy(
            src_ref=src,
            dst_ref=dst,
            send_sem=send,
            recv_sem=recv,
            device_id=(sp, tp),
            device_id_type=pl.DeviceIdType.MESH,
        )

    ring = [(0, 0), (0, 1), (1, 0), (1, 1)]
    clique = [(0, 0), (0, 1), (1, 0), (1, 1)]
    sent = []

    def go(copy):
        copy.start()
        sent.append(copy)

    barrier = pltpu.get_barrier_semaphore()
    for off in range(1, count):
        pl.semaphore_signal(
            barrier,
            inc=1,
            device_id=((me + off) % count, core),
            device_id_type=pl.DeviceIdType.MESH,
        )
    pl.semaphore_signal(
        barrier, inc=1, device_id=(me, 1 - core), device_id_type=pl.DeviceIdType.MESH
    )

    def w_rows(slot):
        q, r = slot // 4, slot % 4
        src = place(*clique[q], *ring[r])
        return pl.ds(pl.multiple_of(src * depth, depth), depth)

    own_x = []
    for s in range(seqs):
        c = pltpu.make_async_copy(
            prompt.at[s], xb.at[0, pl.ds(s * span, span)], local_sem.at[s]
        )
        c.start()
        own_x.append(c)
    kcols = pl.ds(pl.multiple_of(mine * dk, dk), dk)
    vcols = pl.ds(pl.multiple_of(mine * dv, dv), dv)
    own_rows = w_rows(0)
    own_k = pltpu.make_async_copy(w_key.at[:, kcols], wk.at[own_rows], local_sem.at[2])
    own_v = pltpu.make_async_copy(w_value.at[:, vcols], wv.at[own_rows], local_sem.at[3])
    own_k.start()
    own_v.start()
    pl.semaphore_wait(barrier, count)

    for r in (1, 2, 3):
        dz, dx = ring[r]
        peer = place(0, 0, dz, dx)
        theirs = flip(zl, dz) * 2 + flip(x, dx)
        kc = pl.ds(pl.multiple_of(theirs * dk, dk), dk)
        vc = pl.ds(pl.multiple_of(theirs * dv, dv), dv)
        go(remote(w_key.at[:, kc], wk.at[own_rows], wk_send.at[r], wk_recv.at[r], peer, core))
        go(remote(w_value.at[:, vc], wv.at[own_rows], wv_send.at[r], wv_recv.at[r], peer, core))

    def w_relay(slot, to, tag):
        rows = w_rows(slot)
        q = slot // 4
        there = (q + to[0] * 2 + to[1]) * 4 + slot % 4
        peer = place(to[0], to[1], 0, 0)
        go(remote(wk.at[rows], wk.at[rows], wk_send.at[tag], wk_recv.at[there], peer, core))
        go(remote(wv.at[rows], wv.at[rows], wv_send.at[tag], wv_recv.at[there], peer, core))

    def w_wait(slot):
        rows = w_rows(slot)
        pltpu.make_async_copy(wk.at[rows], wk.at[rows], wk_recv.at[slot]).wait()
        pltpu.make_async_copy(wv.at[rows], wv.at[rows], wv_recv.at[slot]).wait()

    def x_part(slot, seq_rows, k):
        return xb.at[slot, seq_rows, pl.ds(k * cut, cut)]

    my_rows = pl.ds(pl.multiple_of(core * span, span), span)
    other_rows = pl.ds(pl.multiple_of((1 - core) * span, span), span)
    to_x, to_z = place(0, 0, 0, 1), place(0, 0, 1, 0)

    def x_send_own(slot, k, peer):
        go(
            remote(
                prompt.at[core, :, pl.ds(k * cut, cut)],
                x_part(slot, my_rows, k),
                x_send.at[slot, k],
                x_recv.at[slot, k],
                peer,
                core,
            )
        )

    def x_wait(slot, k):
        part = x_part(slot, my_rows, k)
        pltpu.make_async_copy(part, part, x_recv.at[slot, k]).wait()

    def x_across(slot, k):
        part = x_part(slot, my_rows, k)
        go(remote(part, part, d_send.at[slot, k], d_recv.at[slot, k], me, 1 - core))

    def d_wait(slot, k):
        part = x_part(slot, other_rows, k)
        pltpu.make_async_copy(part, part, d_recv.at[slot, k]).wait()

    for k in range(PER):
        x_send_own(2, k, to_z)
    for k in range(CHUNKS):
        x_send_own(1, k, to_x)
    own_k.wait()
    own_v.wait()
    w_relay(0, (1, 0), 4)
    w_relay(0, (0, 1), 8)
    for r in (1, 2, 3):
        w_wait(r)
        w_relay(r, (1, 0), 4 + r)
        w_relay(r, (0, 1), 8 + r)
        for k in range(PER):
            x_send_own(2, r * PER + k, to_z)
    for c in own_x:
        c.wait()

    lane = lax.broadcasted_iota(jnp.int32, (seqs * span, 2 * total_heads), 1)
    head = core * heads + mine
    w_gate[...] = jnp.concatenate([w_igate[...], w_fgate[...]], axis=0)
    head_lane = lax.broadcasted_iota(jnp.int32, (1, total_heads), 1) == head
    bias_in = jnp.sum(jnp.where(head_lane, input_bias[...], 0.0), axis=1, keepdims=True)
    bias_f = jnp.sum(jnp.where(head_lane, forget_bias[...], 0.0), axis=1, keepdims=True)
    at_t = lax.broadcasted_iota(jnp.int32, (span, span), 0)
    at_u = lax.broadcasted_iota(jnp.int32, (span, span), 1)
    after = (at_u > at_t).astype(jnp.float32)
    stat_row = lax.broadcasted_iota(jnp.int32, (8, 128), 0)
    stat_lane = lax.broadcasted_iota(jnp.int32, (8, 128), 1)

    def gates(r, table):
        both = lax.dot_general(
            xb[r],
            w_gate[...],
            (((1,), (1,)), ((), ())),
            preferred_element_type=jnp.float32,
        )
        gate_in = bias_in + jnp.sum(jnp.where(lane == head, both, 0.0), axis=1, keepdims=True)
        gate_f = bias_f + jnp.sum(
            jnp.where(lane == total_heads + head, both, 0.0), axis=1, keepdims=True
        )
        forget = log_sigmoid(gate_f)
        for s in range(seqs):
            part = forget[s * span : (s + 1) * span]
            wide = jnp.broadcast_to(part, (span, 128))
            later = jnp.dot(after, wide, precision=HIGH, preferred_element_type=jnp.float32)
            level = later[:, 0:1] + gate_in[s * span : (s + 1) * span]
            top = jnp.max(level, axis=0, keepdims=True)
            total = jnp.sum(part, axis=0, keepdims=True)
            weight[r, s * span : (s + 1) * span] = jnp.broadcast_to(
                jnp.exp(level - top) * key_scale, (span, 128)
            )
            hit = stat_row == r * seqs + s
            table = jnp.where(hit & (stat_lane == 0), total, table)
            table = jnp.where(hit & (stat_lane == 1), top, table)
        return table

    def project(r, slots, first):
        def step(i, carry):
            keys = values = None
            for off in range(2):
                rows = slots(2 * i + off)
                tokens = xb[r, :, rows]
                k_part = jnp.dot(tokens, wk[rows], preferred_element_type=jnp.float32)
                v_part = jnp.dot(tokens, wv[rows], preferred_element_type=jnp.float32)
                keys = k_part if keys is None else keys + k_part
                values = v_part if values is None else values + v_part
            key_acc[r] += keys
            value_acc[r] += values
            return carry

        if first:
            key_acc[r] = jnp.zeros((seqs * span, dk), jnp.float32)
            value_acc[r] = jnp.zeros((seqs * span, dv), jnp.float32)
        return step

    def source_rows(q):
        def rows(r):
            dh, dy = clique[q]
            dz, dx = r // 2, r % 2
            src = place(dh, dy, dz, dx)
            return pl.ds(pl.multiple_of(src * depth, depth), depth)

        return rows

    def group(r, q, first=False):
        lax.fori_loop(0, 2, project(r, source_rows(q), first), 0)

    def finish(r):
        keys = key_acc[r].astype(jnp.bfloat16).astype(jnp.float32)
        decay[r] = (weight[r, :, 0:1] * keys).astype(jnp.bfloat16)
        vals[r] = value_acc[r].astype(jnp.bfloat16)

    table = gates(0, jnp.zeros((8, 128), jnp.float32))
    group(0, 0, True)
    for k in range(4):
        for c in range(k * PER, (k + 1) * PER):
            x_wait(2, c)
            go(
                remote(
                    x_part(2, my_rows, c),
                    x_part(3, my_rows, c),
                    x_send.at[3, c],
                    x_recv.at[3, c],
                    to_x,
                    core,
                )
            )
            x_across(2, c)
        w_wait(8 + k)
        w_relay(8 + k, (0, 1), 12 + k)
        if k == 1:
            for c in range(CHUNKS):
                x_wait(1, c)
                x_across(1, c)
            for slot in range(4, 8):
                w_wait(slot)
            group(0, 1)
        if k == 2:
            for c in range(CHUNKS):
                d_wait(1, c)
            table = gates(1, table)
            group(1, 0, True)
            group(1, 1)
    group(0, 2)
    group(1, 2)
    for c in range(CHUNKS // 2):
        x_wait(3, c)
        x_across(3, c)
    for c in range(CHUNKS):
        d_wait(2, c)
    table = gates(2, table)
    for q in range(3):
        group(2, q, q == 0)
    for c in range(CHUNKS // 2, CHUNKS):
        x_wait(3, c)
        x_across(3, c)
    for slot in range(12, 16):
        w_wait(slot)
    for c in range(CHUNKS):
        d_wait(3, c)
    table = gates(3, table)
    stat[0] = table
    for r in range(3):
        group(r, 3)
        finish(r)
    for q in (1, 2, 3):
        dh, dy = clique[q]
        go(
            remote(
                stat.at[0], stat.at[q], s_send.at[q], s_recv.at[q], place(dh, dy, 0, 0), core
            )
        )
    for q in range(4):
        group(3, q, q == 0)
    finish(3)
    for q in (1, 2, 3):
        pltpu.make_async_copy(stat.at[q], stat.at[q], s_recv.at[q]).wait()

    stats = jnp.concatenate([stat[q] for q in range(4)], axis=0)

    def spot(dim):
        n = lax.broadcasted_iota(jnp.int32, (32, 32), dim)
        dh, dy, dz, dx = n // 16, (n // 8) % 2, (n // 4) % 2, (n // 2) % 2
        where = flip(zh, dh) * 8 + flip(zl, dz) * 4 + flip(y, dy) * 2 + flip(x, dx)
        return where, n % 2

    (pos_a, seq_a), (pos_b, seq_b) = spot(0), spot(1)
    later_mask = ((pos_b > pos_a) & (seq_a == seq_b)).astype(jnp.float32)
    later = jnp.dot(later_mask, stats, precision=HIGH, preferred_element_type=jnp.float32)
    lift = later[:, 0:1] + stats[:, 1:2]
    parity = lax.broadcasted_iota(jnp.int32, (32, 1), 0) % 2
    highest = [
        jnp.max(jnp.where(parity == s, lift, -jnp.inf), axis=0, keepdims=True)
        for s in range(seqs)
    ]
    factor = jnp.exp(lift - jnp.where(parity == 0, highest[0], highest[1]))

    pick = lax.broadcasted_iota(jnp.int32, (heads, dk), 0) == mine
    ones = jnp.ones((8, span), jnp.bfloat16)
    aux_row = lax.broadcasted_iota(jnp.int32, (1, 128), 1)
    tail = jnp.zeros((1, 128), jnp.float32)

    def cut_rows(sp):
        return pl.ds(pl.multiple_of(sp * rows_out, rows_out), rows_out)

    for s in range(seqs):
        sums = jnp.zeros((dk, dv), jnp.float32)
        norms = jnp.zeros((8, dk), jnp.float32)
        for r in range(4):
            d = decay[r, s * span : (s + 1) * span]
            v = vals[r, s * span : (s + 1) * span]
            f = factor[r * seqs + s : r * seqs + s + 1, 0:1]
            sums = sums + f * lax.dot_general(
                d, v, (((0,), (0,)), ((), ())), preferred_element_type=jnp.float32
            )
            norms = norms + f * jnp.dot(ones, d, preferred_element_type=jnp.float32)
        state[s] = sums.astype(jnp.bfloat16)
        query = jnp.sum(
            jnp.where(pick, new_query[s].astype(jnp.float32), 0.0), axis=0, keepdims=True
        )
        seen = jnp.dot(
            jnp.broadcast_to(query, (8, dk)),
            sums,
            precision=HIGH,
            preferred_element_type=jnp.float32,
        )
        for k in range(dv // 128):
            aux[s * 4 + k : s * 4 + k + 1] = seen[0:1, k * 128 : (k + 1) * 128]
        for k in range(dk // 128):
            row = 8 + s * 2 + k
            aux[row : row + 1] = norms[0:1, k * 128 : (k + 1) * 128]
        dot_norm = jnp.sum(query * norms[0:1], axis=1, keepdims=True)
        tail = jnp.where(aux_row == s, highest[s], tail)
        tail = jnp.where(aux_row == 2 + s, dot_norm, tail)
        for off in range(1, count):
            peer = (me + off) % count
            go(
                remote(
                    state.at[s, cut_rows(peer)],
                    rmem.at[me, s],
                    m_send.at[s, off],
                    m_recv.at[s, off],
                    peer,
                    core,
                )
            )
    aux[12:13] = tail
    aux[13:16] = jnp.zeros((3, 128), jnp.float32)
    for off in range(1, count):
        peer = (me + off) % count
        go(remote(aux, raux.at[me], a_send.at[off], a_recv.at[off], peer, core))
    rmem[me] = state[:, cut_rows(me), :]
    raux[me] = aux[...]

    def stack(ref):
        return jnp.concatenate([ref[s].astype(jnp.float32) for s in range(seqs)], axis=0)

    queries = stack(new_query)
    own = jnp.sum(queries * stack(new_key), axis=1, keepdims=True) * key_scale
    own_head = (
        lax.broadcasted_iota(jnp.int32, (seqs * heads, heads), 0) % heads
        == lax.broadcasted_iota(jnp.int32, (seqs * heads, heads), 1)
    )

    def upright(block):
        wide = jnp.concatenate(
            [jnp.broadcast_to(block[s : s + 1], (heads, heads)) for s in range(seqs)], axis=0
        )
        return jnp.sum(jnp.where(own_head, wide, 0.0), axis=1, keepdims=True)

    gate_in, gate_f = upright(new_gates[0]), log_sigmoid(upright(new_gates[1]))
    token_values = stack(new_value)

    for off in range(1, count):
        src = (me + count - off) % count
        for s in range(seqs):
            part = rmem.at[src, s]
            pltpu.make_async_copy(part, part, m_recv.at[s, off]).wait()
        pltpu.make_async_copy(raux.at[src], raux.at[src], a_recv.at[off]).wait()

    read_rows, norm_rows, max_rows, dot_rows = [], [], [], []
    for s in range(seqs):
        for h in range(heads):
            srcs = [
                a * 8 + (h // 2) * 4 + b * 2 + h % 2 for a in range(2) for b in range(2)
            ]
            mem = rmem[srcs[0], s].astype(jnp.float32)
            both = raux[srcs[0]]
            for src in srcs[1:]:
                mem = mem + rmem[src, s].astype(jnp.float32)
                both = both + raux[src]
            memory_out[s, h] = mem.astype(jnp.bfloat16)
            read_rows.append(
                jnp.concatenate([both[s * 4 + k : s * 4 + k + 1] for k in range(dv // 128)], 1)
            )
            norm_rows.append(
                jnp.concatenate(
                    [both[8 + s * 2 + k : 9 + s * 2 + k] for k in range(dk // 128)], 1
                )
            )
            max_rows.append(raux[srcs[0], 12:13, s : s + 1])
            dot_rows.append(both[12:13, 2 + s : 3 + s])
    query_state = jnp.concatenate(read_rows, axis=0)
    norm_all = jnp.concatenate(norm_rows, axis=0)
    top = jnp.concatenate(max_rows, axis=0)
    query_norm = jnp.concatenate(dot_rows, axis=0)
    take = (
        lax.broadcasted_iota(jnp.int32, (dk, rows_out), 0)
        == me * rows_out + lax.broadcasted_iota(jnp.int32, (dk, rows_out), 1)
    ).astype(jnp.float32)
    norm_out[...] = jnp.dot(norm_all, take, precision=HIGH, preferred_element_type=jnp.float32)
    max_out[...] = top
    mixed = jnp.maximum(gate_f + top, gate_in)
    carried = jnp.exp(gate_f + top - mixed)
    fresh = jnp.exp(gate_in - mixed)
    numer = carried * query_state + (fresh * own) * token_values
    denom = carried * query_norm + fresh * own
    read_out[...] = (numer / jnp.maximum(jnp.abs(denom), 1.0)).astype(jnp.bfloat16)
    for copy in sent:
        copy.wait_send()


def hand_on(memory, norm, top, read, memory_out, norm_out, max_out, read_out):
    seqs, heads = max_out.shape
    memory_out[...] = memory[...]
    at = lax.broadcasted_iota(jnp.int32, (seqs * heads, heads), 0)
    to = lax.broadcasted_iota(jnp.int32, (seqs * heads, heads), 1)
    wide = read[...].astype(jnp.float32)
    for s in range(seqs):
        rows = slice(s * heads, (s + 1) * heads)
        norm_out[s] = norm[rows]
        read_out[s] = wide[rows].astype(jnp.bfloat16)
        max_out[s : s + 1] = jnp.sum(
            jnp.where(at == s * heads + to, top[...], 0.0), axis=0, keepdims=True
        )


def by_head(
    prompt,
    w_key,
    w_value,
    w_igate,
    w_fgate,
    input_bias,
    forget_bias,
    new_query,
    new_key,
    new_value,
    new_gates,
):
    count = lax.axis_size("sp")
    seqs, span, width = prompt.shape
    depth = w_key.shape[0]
    heads, dk = new_query.shape[1:]
    dv = new_value.shape[2]
    rows = seqs * span
    vmem = pl.BlockSpec(memory_space=pltpu.VMEM)
    hbm = pl.BlockSpec(memory_space=pl.ANY)
    dma = pltpu.SemaphoreType.DMA
    memory, norm, top, read = pl.pallas_call(
        kernel,
        out_shape=(
            jax.ShapeDtypeStruct((seqs, heads, dk // count, dv), jnp.bfloat16),
            jax.ShapeDtypeStruct((seqs * heads, dk // count), jnp.float32),
            jax.ShapeDtypeStruct((seqs * heads, 1), jnp.float32),
            jax.ShapeDtypeStruct((seqs * heads, dv), jnp.bfloat16),
        ),
        in_specs=[hbm, hbm, hbm] + [vmem] * 8,
        out_specs=(vmem, vmem, vmem, vmem),
        scratch_shapes=[
            pltpu.VMEM((4, rows, width), jnp.bfloat16),
            pltpu.VMEM((width, dk), jnp.bfloat16),
            pltpu.VMEM((width, dv), jnp.bfloat16),
            pltpu.VMEM((2 * w_igate.shape[1], width), jnp.bfloat16),
            pltpu.VMEM((4, rows, dk), jnp.float32),
            pltpu.VMEM((4, rows, dv), jnp.float32),
            pltpu.VMEM((4, rows, dk), jnp.bfloat16),
            pltpu.VMEM((4, rows, dv), jnp.bfloat16),
            pltpu.VMEM((4, rows, 128), jnp.float32),
            pltpu.VMEM((4, 8, 128), jnp.float32),
            pltpu.VMEM((seqs, dk, dv), jnp.bfloat16),
            pltpu.VMEM((16, 128), jnp.float32),
            pltpu.VMEM((count, seqs, dk // count, dv), jnp.bfloat16),
            pltpu.VMEM((count, 16, 128), jnp.float32),
            dma((4,)),
            dma((4, CHUNKS)),
            dma((4, CHUNKS)),
            dma((4, CHUNKS)),
            dma((4, CHUNKS)),
            dma((16,)),
            dma((16,)),
            dma((16,)),
            dma((16,)),
            dma((4,)),
            dma((4,)),
            dma((seqs, count)),
            dma((seqs, count)),
            dma((count,)),
            dma((count,)),
        ],
        compiler_params=pltpu.CompilerParams(
            collective_id=0, has_side_effects=True, vmem_limit_bytes=60 * 1024 * 1024
        ),
    )(
        prompt,
        w_key,
        w_value,
        w_igate.T,
        w_fgate.T,
        input_bias[None],
        forget_bias[None],
        new_query,
        new_key,
        new_value,
        new_gates,
    )
    return pl.pallas_call(
        hand_on,
        out_shape=(
            jax.ShapeDtypeStruct((seqs, heads, dk // count, dv), jnp.bfloat16),
            jax.ShapeDtypeStruct((seqs, heads, dk // count), jnp.float32),
            jax.ShapeDtypeStruct((seqs, heads), jnp.float32),
            jax.ShapeDtypeStruct((seqs, heads, dv), jnp.bfloat16),
        ),
        in_specs=[vmem] * 4,
        out_specs=(vmem,) * 4,
    )(memory, norm, top, read)


def chosen(*args):
    prompt, new_query, new_value = args[0], args[7], args[9]
    heads = new_query.shape[1]
    count = lax.axis_size("sp")
    fits = (
        lax.axis_size("tp") == 2
        and heads == 4
        and count == 16
        and prompt.shape[0] == 2
        and new_query.shape[2] == 256
        and new_value.shape[2] == 512
    )
    return by_head(*args) if fits else per_device(*args)


def entering(value, axis, join, neutral):
    count, mine = (lax.axis_size(axis), lax.axis_index(axis))
    pieces = lax.all_gather(value, axis)
    pieces = pieces[::-1]
    mine = count - 1 - mine
    so_far = jnp.full_like(value, 0) + jnp.asarray(neutral, value.dtype)

    def turn(position, so_far):
        longer = join(so_far, pieces[position])
        return jnp.where(position < mine, longer, so_far)

    return lax.fori_loop(0, count - 1, turn, so_far)


def add_pair(earlier, later):
    return earlier + later


def per_device(
    prompt,
    w_key,
    w_value,
    w_igate,
    w_fgate,
    input_bias,
    forget_bias,
    new_query,
    new_key,
    new_value,
    new_gates,
):
    seq_count, span_len, model_width = prompt.shape
    local_heads = new_query.shape[1]
    key_size = new_query.shape[2]
    value_size = new_value.shape[2]
    key_scale = key_size ** (-0.5)
    token_rows = prompt.reshape(seq_count * span_len, model_width)
    whole_key, whole_value = (
        lax.all_gather(w_key, "sp", axis=0, tiled=True),
        lax.all_gather(w_value, "sp", axis=0, tiled=True),
    )
    key_rows = jnp.dot(token_rows, whole_key, preferred_element_type=jnp.float32).astype(
        jnp.bfloat16
    )
    value_rows = jnp.dot(token_rows, whole_value, preferred_element_type=jnp.float32).astype(
        jnp.bfloat16
    )
    head_start = lax.axis_index("tp") * local_heads
    input_all = jnp.dot(token_rows, w_igate, preferred_element_type=jnp.float32) + input_bias
    forget_all = jnp.dot(token_rows, w_fgate, preferred_element_type=jnp.float32) + forget_bias
    input_gate = lax.dynamic_slice_in_dim(input_all, head_start, local_heads, 1).reshape(
        seq_count, span_len, local_heads
    )
    log_forget = jax.nn.log_sigmoid(
        lax.dynamic_slice_in_dim(forget_all, head_start, local_heads, 1)
    ).reshape(seq_count, span_len, local_heads)
    block_total = jnp.sum(log_forget, axis=1)
    forget_after = block_total[:, None] - jnp.cumsum(log_forget, axis=1)
    log_weight = forget_after + input_gate
    block_max = jnp.max(log_weight, axis=1)
    key_blocks = key_rows.reshape(seq_count, span_len, local_heads, key_size).astype(jnp.float32)
    decayed = (jnp.exp(log_weight - block_max[:, None])[..., None] * key_scale * key_blocks).astype(
        jnp.bfloat16
    )
    value_blocks = value_rows.reshape(seq_count, span_len, local_heads, value_size)
    block_norm = jnp.sum(decayed.astype(jnp.float32), axis=1)
    later_total = entering(block_total, "sp", add_pair, jnp.zeros_like(block_total))
    block_lift = later_total + block_max
    global_max = lax.pmax(block_lift, "sp")
    factor = jnp.exp(block_lift - global_max)
    scaled_norm = factor[:, :, None] * block_norm
    query_full = new_query.astype(jnp.float32)
    block_state = jnp.einsum(
        "sthk,sthv->shkv", decayed, value_blocks, preferred_element_type=jnp.float32
    )
    scaled_state = factor[:, :, None, None] * block_state
    memory_rows, norm_rows = (
        lax.psum_scatter(scaled_state, "sp", scatter_dimension=2, tiled=True),
        lax.psum_scatter(scaled_norm, "sp", scatter_dimension=2, tiled=True),
    )
    token_score = jnp.einsum(
        "shk,sthk->sth", new_query, decayed, preferred_element_type=jnp.float32
    )
    score_high = token_score.astype(jnp.bfloat16)
    score_low = (token_score - score_high.astype(jnp.float32)).astype(jnp.bfloat16)
    weighted = jnp.einsum(
        "sth,sthv->shv", score_high, value_blocks, preferred_element_type=jnp.float32
    )
    weighted = weighted + jnp.einsum(
        "sth,sthv->shv", score_low, value_blocks, preferred_element_type=jnp.float32
    )
    partial_state = factor[..., None] * weighted
    partial_norm = jnp.sum(query_full * scaled_norm, axis=-1)
    query_state, query_norm = lax.psum((partial_state, partial_norm), "sp")
    forget_new = jax.nn.log_sigmoid(new_gates[1])
    input_new = new_gates[0]
    mixed = jnp.maximum(forget_new + global_max, input_new)
    carried = jnp.exp(forget_new + global_max - mixed)
    fresh = jnp.exp(input_new - mixed)
    own_score = jnp.sum(query_full * new_key.astype(jnp.float32), axis=-1) * key_scale
    numer = carried[..., None] * query_state + (fresh * own_score)[..., None] * new_value.astype(
        jnp.float32
    )
    denom = carried * query_norm + fresh * own_score
    first_read = (numer / jnp.maximum(jnp.abs(denom), 1.0)[..., None]).astype(jnp.bfloat16)
    return (memory_rows.astype(jnp.bfloat16), norm_rows, global_max, first_read)


def solution(mesh):
    placed = (
        P(None, "sp", None),
        P("sp", "tp"),
        P("sp", "tp"),
        P(),
        P(),
        P(),
        P(),
        P(None, "tp", None),
        P(None, "tp", None),
        P(None, "tp", None),
        P(None, None, "tp"),
    )
    return jax.shard_map(
        chosen,
        mesh=mesh,
        in_specs=placed,
        out_specs=(
            P(None, "tp", "sp", None),
            P(None, "tp", "sp"),
            P(None, "tp"),
            P(None, "tp", None),
        ),
        check_vma=False,
    )
```

```python
import functools
import jax
import jax.numpy as jnp
from jax import lax
from jax.experimental import pallas as pl
from jax.experimental.pallas import tpu as pltpu
from jax.sharding import PartitionSpec as P

CHUNKS = 8
PER = CHUNKS // 4
HIGH = lax.Precision.HIGHEST


def flip(bit, change):
    return bit + change - 2 * bit * change


def log_sigmoid(v):
    return jnp.minimum(v, 0.0) - jnp.log1p(jnp.exp(-jnp.abs(v)))


def kernel(
    prompt,
    w_key,
    w_value,
    w_igate,
    w_fgate,
    input_bias,
    forget_bias,
    new_query,
    new_key,
    new_value,
    new_gates,
    memory_out,
    norm_out,
    max_out,
    read_out,
    xb,
    wk,
    wv,
    w_gate,
    key_acc,
    value_acc,
    decay,
    vals,
    weight,
    stat,
    state,
    aux,
    yin,
    yaux,
    total_state,
    total_aux,
    rmem,
    raux,
    local_sem,
    x_send,
    x_recv,
    d_send,
    d_recv,
    wk_send,
    wk_recv,
    wv_send,
    wv_recv,
    s_send,
    s_recv,
    y_send,
    y_recv,
    m_send,
    m_recv,
    a_send,
    a_recv,
):
    count = lax.axis_size("sp")
    me = lax.axis_index("sp")
    core = lax.axis_index("tp")
    seqs, span, width = prompt.shape
    depth = w_key.shape[0]
    heads = new_query.shape[1]
    dk = new_query.shape[2]
    dv = new_value.shape[2]
    total_heads = input_bias.shape[1]
    key_scale = dk ** (-0.5)
    cut = width // CHUNKS
    rows_out = dk // count
    zh, zl, y, x = me // 8, (me // 4) % 2, (me // 2) % 2, me % 2
    mine = zl * 2 + x

    def place(dh, dy, dz, dx):
        return flip(zh, dh) * 8 + flip(zl, dz) * 4 + flip(y, dy) * 2 + flip(x, dx)

    def remote(src, dst, send, recv, sp, tp):
        return pltpu.make_async_remote_copy(
            src_ref=src,
            dst_ref=dst,
            send_sem=send,
            recv_sem=recv,
            device_id=(sp, tp),
            device_id_type=pl.DeviceIdType.MESH,
        )

    ring = [(0, 0), (0, 1), (1, 0), (1, 1)]
    clique = [(0, 0), (0, 1), (1, 0), (1, 1)]
    sent = []

    def go(copy):
        copy.start()
        sent.append(copy)

    barrier = pltpu.get_barrier_semaphore()
    for off in range(1, count):
        pl.semaphore_signal(
            barrier,
            inc=1,
            device_id=((me + off) % count, core),
            device_id_type=pl.DeviceIdType.MESH,
        )
    pl.semaphore_signal(
        barrier, inc=1, device_id=(me, 1 - core), device_id_type=pl.DeviceIdType.MESH
    )

    def w_rows(slot):
        q, r = slot // 4, slot % 4
        src = place(*clique[q], *ring[r])
        return pl.ds(pl.multiple_of(src * depth, depth), depth)

    own_x = []
    for s in range(seqs):
        c = pltpu.make_async_copy(
            prompt.at[s], xb.at[0, pl.ds(s * span, span)], local_sem.at[s]
        )
        c.start()
        own_x.append(c)
    kcols = pl.ds(pl.multiple_of(mine * dk, dk), dk)
    vcols = pl.ds(pl.multiple_of(mine * dv, dv), dv)
    own_rows = w_rows(0)
    own_k = pltpu.make_async_copy(w_key.at[:, kcols], wk.at[own_rows], local_sem.at[2])
    own_v = pltpu.make_async_copy(w_value.at[:, vcols], wv.at[own_rows], local_sem.at[3])
    own_k.start()
    own_v.start()
    pl.semaphore_wait(barrier, count)

    for r in (1, 2, 3):
        dz, dx = ring[r]
        peer = place(0, 0, dz, dx)
        theirs = flip(zl, dz) * 2 + flip(x, dx)
        kc = pl.ds(pl.multiple_of(theirs * dk, dk), dk)
        vc = pl.ds(pl.multiple_of(theirs * dv, dv), dv)
        go(remote(w_key.at[:, kc], wk.at[own_rows], wk_send.at[r], wk_recv.at[r], peer, core))
        go(remote(w_value.at[:, vc], wv.at[own_rows], wv_send.at[r], wv_recv.at[r], peer, core))

    def w_relay(slot, to, tag):
        rows = w_rows(slot)
        q = slot // 4
        there = (q + to[0] * 2 + to[1]) * 4 + slot % 4
        peer = place(to[0], to[1], 0, 0)
        go(remote(wk.at[rows], wk.at[rows], wk_send.at[tag], wk_recv.at[there], peer, core))
        go(remote(wv.at[rows], wv.at[rows], wv_send.at[tag], wv_recv.at[there], peer, core))

    def w_wait(slot):
        rows = w_rows(slot)
        pltpu.make_async_copy(wk.at[rows], wk.at[rows], wk_recv.at[slot]).wait()
        pltpu.make_async_copy(wv.at[rows], wv.at[rows], wv_recv.at[slot]).wait()

    def x_part(slot, seq_rows, k):
        return xb.at[slot, seq_rows, pl.ds(k * cut, cut)]

    my_rows = pl.ds(pl.multiple_of(core * span, span), span)
    other_rows = pl.ds(pl.multiple_of((1 - core) * span, span), span)
    to_x, to_z = place(0, 0, 0, 1), place(0, 0, 1, 0)

    def x_send_own(slot, k, peer):
        go(
            remote(
                prompt.at[core, :, pl.ds(k * cut, cut)],
                x_part(slot, my_rows, k),
                x_send.at[slot, k],
                x_recv.at[slot, k],
                peer,
                core,
            )
        )

    def x_wait(slot, k):
        part = x_part(slot, my_rows, k)
        pltpu.make_async_copy(part, part, x_recv.at[slot, k]).wait()

    def x_across(slot, k):
        part = x_part(slot, my_rows, k)
        go(remote(part, part, d_send.at[slot, k], d_recv.at[slot, k], me, 1 - core))

    def d_wait(slot, k):
        part = x_part(slot, other_rows, k)
        pltpu.make_async_copy(part, part, d_recv.at[slot, k]).wait()

    for k in range(PER):
        x_send_own(2, k, to_z)
    for k in range(CHUNKS):
        x_send_own(1, k, to_x)
    own_k.wait()
    own_v.wait()
    w_relay(0, (1, 0), 4)
    w_relay(0, (0, 1), 8)
    for r in (1, 2, 3):
        w_wait(r)
        w_relay(r, (1, 0), 4 + r)
        w_relay(r, (0, 1), 8 + r)
        for k in range(PER):
            x_send_own(2, r * PER + k, to_z)
    for c in own_x:
        c.wait()

    lane = lax.broadcasted_iota(jnp.int32, (seqs * span, 2 * total_heads), 1)
    head = core * heads + mine
    w_gate[...] = jnp.concatenate([w_igate[...], w_fgate[...]], axis=0)
    head_lane = lax.broadcasted_iota(jnp.int32, (1, total_heads), 1) == head
    bias_in = jnp.sum(jnp.where(head_lane, input_bias[...], 0.0), axis=1, keepdims=True)
    bias_f = jnp.sum(jnp.where(head_lane, forget_bias[...], 0.0), axis=1, keepdims=True)
    at_t = lax.broadcasted_iota(jnp.int32, (span, span), 0)
    at_u = lax.broadcasted_iota(jnp.int32, (span, span), 1)
    after = (at_u > at_t).astype(jnp.float32)
    stat_row = lax.broadcasted_iota(jnp.int32, (8, 128), 0)
    stat_lane = lax.broadcasted_iota(jnp.int32, (8, 128), 1)

    def gates(r, table):
        both = lax.dot_general(
            xb[r],
            w_gate[...],
            (((1,), (1,)), ((), ())),
            preferred_element_type=jnp.float32,
        )
        gate_in = bias_in + jnp.sum(jnp.where(lane == head, both, 0.0), axis=1, keepdims=True)
        gate_f = bias_f + jnp.sum(
            jnp.where(lane == total_heads + head, both, 0.0), axis=1, keepdims=True
        )
        forget = log_sigmoid(gate_f)
        for s in range(seqs):
            part = forget[s * span : (s + 1) * span]
            wide = jnp.broadcast_to(part, (span, 128))
            later = jnp.dot(after, wide, precision=HIGH, preferred_element_type=jnp.float32)
            level = later[:, 0:1] + gate_in[s * span : (s + 1) * span]
            top = jnp.max(level, axis=0, keepdims=True)
            total = jnp.sum(part, axis=0, keepdims=True)
            weight[r, s * span : (s + 1) * span] = jnp.broadcast_to(
                jnp.exp(level - top) * key_scale, (span, 128)
            )
            hit = stat_row == r * seqs + s
            table = jnp.where(hit & (stat_lane == 0), total, table)
            table = jnp.where(hit & (stat_lane == 1), top, table)
        return table

    def project(r, slots, first):
        def step(i, carry):
            keys = values = None
            for off in range(2):
                rows = slots(2 * i + off)
                tokens = xb[r, :, rows]
                k_part = jnp.dot(tokens, wk[rows], preferred_element_type=jnp.float32)
                v_part = jnp.dot(tokens, wv[rows], preferred_element_type=jnp.float32)
                keys = k_part if keys is None else keys + k_part
                values = v_part if values is None else values + v_part
            key_acc[r] += keys
            value_acc[r] += values
            return carry

        if first:
            key_acc[r] = jnp.zeros((seqs * span, dk), jnp.float32)
            value_acc[r] = jnp.zeros((seqs * span, dv), jnp.float32)
        return step

    def source_rows(q):
        def rows(r):
            dh, dy = clique[q]
            dz, dx = r // 2, r % 2
            src = place(dh, dy, dz, dx)
            return pl.ds(pl.multiple_of(src * depth, depth), depth)

        return rows

    def group(r, q, first=False):
        lax.fori_loop(0, 2, project(r, source_rows(q), first), 0)

    def finish(r):
        keys = key_acc[r].astype(jnp.bfloat16).astype(jnp.float32)
        decay[r] = (weight[r, :, 0:1] * keys).astype(jnp.bfloat16)
        vals[r] = value_acc[r].astype(jnp.bfloat16)

    table = gates(0, jnp.zeros((8, 128), jnp.float32))
    group(0, 0, True)
    for k in range(4):
        for c in range(k * PER, (k + 1) * PER):
            x_wait(2, c)
            go(
                remote(
                    x_part(2, my_rows, c),
                    x_part(3, my_rows, c),
                    x_send.at[3, c],
                    x_recv.at[3, c],
                    to_x,
                    core,
                )
            )
            x_across(2, c)
        w_wait(8 + k)
        w_relay(8 + k, (0, 1), 12 + k)
        if k == 1:
            for c in range(CHUNKS):
                x_wait(1, c)
                x_across(1, c)
            for slot in range(4, 8):
                w_wait(slot)
            group(0, 1)
        if k == 2:
            for c in range(CHUNKS):
                d_wait(1, c)
            table = gates(1, table)
            group(1, 0, True)
            group(1, 1)
    group(0, 2)
    group(1, 2)
    for c in range(CHUNKS // 2):
        x_wait(3, c)
        x_across(3, c)
    for c in range(CHUNKS):
        d_wait(2, c)
    table = gates(2, table)
    for q in range(3):
        group(2, q, q == 0)
    for c in range(CHUNKS // 2, CHUNKS):
        x_wait(3, c)
        x_across(3, c)
    for slot in range(12, 16):
        w_wait(slot)
    for c in range(CHUNKS):
        d_wait(3, c)
    table = gates(3, table)
    stat[0] = table
    for r in range(3):
        group(r, 3)
        finish(r)
    for q in (1, 2, 3):
        dh, dy = clique[q]
        go(
            remote(
                stat.at[0], stat.at[q], s_send.at[q], s_recv.at[q], place(dh, dy, 0, 0), core
            )
        )
    for q in range(4):
        group(3, q, q == 0)
    finish(3)
    for q in (1, 2, 3):
        pltpu.make_async_copy(stat.at[q], stat.at[q], s_recv.at[q]).wait()

    stats = jnp.concatenate([stat[q] for q in range(4)], axis=0)

    def spot(dim):
        n = lax.broadcasted_iota(jnp.int32, (32, 32), dim)
        dh, dy, dz, dx = n // 16, (n // 8) % 2, (n // 4) % 2, (n // 2) % 2
        where = flip(zh, dh) * 8 + flip(zl, dz) * 4 + flip(y, dy) * 2 + flip(x, dx)
        return where, n % 2

    (pos_a, seq_a), (pos_b, seq_b) = spot(0), spot(1)
    later_mask = ((pos_b > pos_a) & (seq_a == seq_b)).astype(jnp.float32)
    later = jnp.dot(later_mask, stats, precision=HIGH, preferred_element_type=jnp.float32)
    lift = later[:, 0:1] + stats[:, 1:2]
    parity = lax.broadcasted_iota(jnp.int32, (32, 1), 0) % 2
    highest = [
        jnp.max(jnp.where(parity == s, lift, -jnp.inf), axis=0, keepdims=True)
        for s in range(seqs)
    ]
    factor = jnp.exp(lift - jnp.where(parity == 0, highest[0], highest[1]))

    pick = lax.broadcasted_iota(jnp.int32, (heads, dk), 0) == mine
    ones = jnp.ones((8, span), jnp.bfloat16)
    aux_row = lax.broadcasted_iota(jnp.int32, (1, 128), 1)
    tail = jnp.zeros((1, 128), jnp.float32)

    to_y = place(0, 1, 0, 0)
    half = count // 2
    spot8 = (zh * 2 + zl) * 2 + x

    def cut_rows(spot):
        return pl.ds(pl.multiple_of(spot * rows_out, rows_out), rows_out)

    for s in range(seqs):
        sums = jnp.zeros((dk, dv), jnp.float32)
        norms = jnp.zeros((8, dk), jnp.float32)
        for r in range(4):
            d = decay[r, s * span : (s + 1) * span]
            v = vals[r, s * span : (s + 1) * span]
            f = factor[r * seqs + s : r * seqs + s + 1, 0:1]
            sums = sums + f * lax.dot_general(
                d, v, (((0,), (0,)), ((), ())), preferred_element_type=jnp.float32
            )
            norms = norms + f * jnp.dot(ones, d, preferred_element_type=jnp.float32)
        for block in range(count // 2):
            rows = sums[block * 2 * rows_out : (block + 1) * 2 * rows_out]
            low = (block // 2) * 2 * rows_out
            state[s, block % 2, low : low + 2 * rows_out] = rows.astype(jnp.bfloat16)
        query = jnp.sum(
            jnp.where(pick, new_query[s].astype(jnp.float32), 0.0), axis=0, keepdims=True
        )
        seen = jnp.dot(
            jnp.broadcast_to(query, (8, dk)),
            sums,
            precision=HIGH,
            preferred_element_type=jnp.float32,
        )
        for k in range(dv // 128):
            aux[s * 4 + k : s * 4 + k + 1] = seen[0:1, k * 128 : (k + 1) * 128]
        for k in range(dk // 128):
            row = 8 + s * 2 + k
            aux[row : row + 1] = norms[0:1, k * 128 : (k + 1) * 128]
        dot_norm = jnp.sum(query * norms[0:1], axis=1, keepdims=True)
        tail = jnp.where(aux_row == s, highest[s], tail)
        tail = jnp.where(aux_row == 2 + s, dot_norm, tail)
        go(
            remote(state.at[s, 1 - y], yin.at[s], y_send.at[s], y_recv.at[s], to_y, core)
        )
    aux[12:13] = tail
    aux[13:16] = jnp.zeros((3, 128), jnp.float32)
    go(remote(aux, yaux, y_send.at[2], y_recv.at[2], to_y, core))

    def of_spot(spot):
        return (spot // 2) * 4 + y * 2 + spot % 2

    for s in range(seqs):
        pltpu.make_async_copy(yin.at[s], yin.at[s], y_recv.at[s]).wait()
        total_state[s] = (
            state[s, y].astype(jnp.float32) + yin[s].astype(jnp.float32)
        ).astype(jnp.bfloat16)
        for off in range(1, half):
            spot = (spot8 + off) % half
            go(
                remote(
                    total_state.at[s, cut_rows(spot)],
                    rmem.at[spot8, s],
                    m_send.at[s, off],
                    m_recv.at[s, off],
                    of_spot(spot),
                    core,
                )
            )
        rmem[spot8, s] = total_state[s, cut_rows(spot8), :]
    pltpu.make_async_copy(yaux, yaux, y_recv.at[2]).wait()
    keep = (lax.broadcasted_iota(jnp.int32, (16, 128), 0) == 12) & (
        lax.broadcasted_iota(jnp.int32, (16, 128), 1) < seqs
    )
    total_aux[...] = jnp.where(keep, aux[...], aux[...] + yaux[...])
    for off in range(1, half):
        go(
            remote(
                total_aux,
                raux.at[spot8],
                a_send.at[off],
                a_recv.at[off],
                of_spot((spot8 + off) % half),
                core,
            )
        )
    raux[spot8] = total_aux[...]

    def stack(ref):
        return jnp.concatenate([ref[s].astype(jnp.float32) for s in range(seqs)], axis=0)

    queries = stack(new_query)
    own = jnp.sum(queries * stack(new_key), axis=1, keepdims=True) * key_scale
    own_head = (
        lax.broadcasted_iota(jnp.int32, (seqs * heads, heads), 0) % heads
        == lax.broadcasted_iota(jnp.int32, (seqs * heads, heads), 1)
    )

    def upright(block):
        wide = jnp.concatenate(
            [jnp.broadcast_to(block[s : s + 1], (heads, heads)) for s in range(seqs)], axis=0
        )
        return jnp.sum(jnp.where(own_head, wide, 0.0), axis=1, keepdims=True)

    gate_in, gate_f = upright(new_gates[0]), log_sigmoid(upright(new_gates[1]))
    token_values = stack(new_value)

    for off in range(1, half):
        src = (spot8 + half - off) % half
        for s in range(seqs):
            part = rmem.at[src, s]
            pltpu.make_async_copy(part, part, m_recv.at[s, off]).wait()
        pltpu.make_async_copy(raux.at[src], raux.at[src], a_recv.at[off]).wait()

    read_rows, norm_rows, max_rows, dot_rows = [], [], [], []
    for s in range(seqs):
        for h in range(heads):
            srcs = [(a * 2 + h // 2) * 2 + h % 2 for a in range(2)]
            mem = rmem[srcs[0], s].astype(jnp.float32)
            both = raux[srcs[0]]
            for src in srcs[1:]:
                mem = mem + rmem[src, s].astype(jnp.float32)
                both = both + raux[src]
            memory_out[s, h] = mem.astype(jnp.bfloat16)
            read_rows.append(
                jnp.concatenate([both[s * 4 + k : s * 4 + k + 1] for k in range(dv // 128)], 1)
            )
            norm_rows.append(
                jnp.concatenate(
                    [both[8 + s * 2 + k : 9 + s * 2 + k] for k in range(dk // 128)], 1
                )
            )
            max_rows.append(raux[srcs[0], 12:13, s : s + 1])
            dot_rows.append(both[12:13, 2 + s : 3 + s])
    query_state = jnp.concatenate(read_rows, axis=0)
    norm_all = jnp.concatenate(norm_rows, axis=0)
    top = jnp.concatenate(max_rows, axis=0)
    query_norm = jnp.concatenate(dot_rows, axis=0)
    take = (
        lax.broadcasted_iota(jnp.int32, (dk, rows_out), 0)
        == me * rows_out + lax.broadcasted_iota(jnp.int32, (dk, rows_out), 1)
    ).astype(jnp.float32)
    norm_out[...] = jnp.dot(norm_all, take, precision=HIGH, preferred_element_type=jnp.float32)
    max_out[...] = top
    mixed = jnp.maximum(gate_f + top, gate_in)
    carried = jnp.exp(gate_f + top - mixed)
    fresh = jnp.exp(gate_in - mixed)
    numer = carried * query_state + (fresh * own) * token_values
    denom = carried * query_norm + fresh * own
    read_out[...] = (numer / jnp.maximum(jnp.abs(denom), 1.0)).astype(jnp.bfloat16)
    for copy in sent:
        copy.wait_send()


def hand_on(memory, norm, top, read, memory_out, norm_out, max_out, read_out):
    seqs, heads = max_out.shape
    memory_out[...] = memory[...]
    at = lax.broadcasted_iota(jnp.int32, (seqs * heads, heads), 0)
    to = lax.broadcasted_iota(jnp.int32, (seqs * heads, heads), 1)
    wide = read[...].astype(jnp.float32)
    for s in range(seqs):
        rows = slice(s * heads, (s + 1) * heads)
        norm_out[s] = norm[rows]
        read_out[s] = wide[rows].astype(jnp.bfloat16)
        max_out[s : s + 1] = jnp.sum(
            jnp.where(at == s * heads + to, top[...], 0.0), axis=0, keepdims=True
        )


def by_head(
    prompt,
    w_key,
    w_value,
    w_igate,
    w_fgate,
    input_bias,
    forget_bias,
    new_query,
    new_key,
    new_value,
    new_gates,
):
    count = lax.axis_size("sp")
    seqs, span, width = prompt.shape
    depth = w_key.shape[0]
    heads, dk = new_query.shape[1:]
    dv = new_value.shape[2]
    rows = seqs * span
    vmem = pl.BlockSpec(memory_space=pltpu.VMEM)
    hbm = pl.BlockSpec(memory_space=pl.ANY)
    dma = pltpu.SemaphoreType.DMA
    memory, norm, top, read = pl.pallas_call(
        kernel,
        out_shape=(
            jax.ShapeDtypeStruct((seqs, heads, dk // count, dv), jnp.bfloat16),
            jax.ShapeDtypeStruct((seqs * heads, dk // count), jnp.float32),
            jax.ShapeDtypeStruct((seqs * heads, 1), jnp.float32),
            jax.ShapeDtypeStruct((seqs * heads, dv), jnp.bfloat16),
        ),
        in_specs=[hbm, hbm, hbm] + [vmem] * 8,
        out_specs=(vmem, vmem, vmem, vmem),
        scratch_shapes=[
            pltpu.VMEM((4, rows, width), jnp.bfloat16),
            pltpu.VMEM((width, dk), jnp.bfloat16),
            pltpu.VMEM((width, dv), jnp.bfloat16),
            pltpu.VMEM((2 * w_igate.shape[1], width), jnp.bfloat16),
            pltpu.VMEM((4, rows, dk), jnp.float32),
            pltpu.VMEM((4, rows, dv), jnp.float32),
            pltpu.VMEM((4, rows, dk), jnp.bfloat16),
            pltpu.VMEM((4, rows, dv), jnp.bfloat16),
            pltpu.VMEM((4, rows, 128), jnp.float32),
            pltpu.VMEM((4, 8, 128), jnp.float32),
            pltpu.VMEM((seqs, 2, dk // 2, dv), jnp.bfloat16),
            pltpu.VMEM((16, 128), jnp.float32),
            pltpu.VMEM((seqs, dk // 2, dv), jnp.bfloat16),
            pltpu.VMEM((16, 128), jnp.float32),
            pltpu.VMEM((seqs, dk // 2, dv), jnp.bfloat16),
            pltpu.VMEM((16, 128), jnp.float32),
            pltpu.VMEM((count // 2, seqs, dk // count, dv), jnp.bfloat16),
            pltpu.VMEM((count // 2, 16, 128), jnp.float32),
            dma((4,)),
            dma((4, CHUNKS)),
            dma((4, CHUNKS)),
            dma((4, CHUNKS)),
            dma((4, CHUNKS)),
            dma((16,)),
            dma((16,)),
            dma((16,)),
            dma((16,)),
            dma((4,)),
            dma((4,)),
            dma((3,)),
            dma((3,)),
            dma((seqs, count)),
            dma((seqs, count)),
            dma((count,)),
            dma((count,)),
        ],
        compiler_params=pltpu.CompilerParams(
            collective_id=0, has_side_effects=True, vmem_limit_bytes=60 * 1024 * 1024
        ),
    )(
        prompt,
        w_key,
        w_value,
        w_igate.T,
        w_fgate.T,
        input_bias[None],
        forget_bias[None],
        new_query,
        new_key,
        new_value,
        new_gates,
    )
    return pl.pallas_call(
        hand_on,
        out_shape=(
            jax.ShapeDtypeStruct((seqs, heads, dk // count, dv), jnp.bfloat16),
            jax.ShapeDtypeStruct((seqs, heads, dk // count), jnp.float32),
            jax.ShapeDtypeStruct((seqs, heads), jnp.float32),
            jax.ShapeDtypeStruct((seqs, heads, dv), jnp.bfloat16),
        ),
        in_specs=[vmem] * 4,
        out_specs=(vmem,) * 4,
    )(memory, norm, top, read)


def chosen(*args):
    prompt, new_query, new_value = args[0], args[7], args[9]
    heads = new_query.shape[1]
    count = lax.axis_size("sp")
    fits = (
        lax.axis_size("tp") == 2
        and heads == 4
        and count == 16
        and prompt.shape[0] == 2
        and new_query.shape[2] == 256
        and new_value.shape[2] == 512
    )
    return by_head(*args) if fits else per_device(*args)


def entering(value, axis, join, neutral):
    count, mine = (lax.axis_size(axis), lax.axis_index(axis))
    pieces = lax.all_gather(value, axis)
    pieces = pieces[::-1]
    mine = count - 1 - mine
    so_far = jnp.full_like(value, 0) + jnp.asarray(neutral, value.dtype)

    def turn(position, so_far):
        longer = join(so_far, pieces[position])
        return jnp.where(position < mine, longer, so_far)

    return lax.fori_loop(0, count - 1, turn, so_far)


def add_pair(earlier, later):
    return earlier + later


def per_device(
    prompt,
    w_key,
    w_value,
    w_igate,
    w_fgate,
    input_bias,
    forget_bias,
    new_query,
    new_key,
    new_value,
    new_gates,
):
    seq_count, span_len, model_width = prompt.shape
    local_heads = new_query.shape[1]
    key_size = new_query.shape[2]
    value_size = new_value.shape[2]
    key_scale = key_size ** (-0.5)
    token_rows = prompt.reshape(seq_count * span_len, model_width)
    whole_key, whole_value = (
        lax.all_gather(w_key, "sp", axis=0, tiled=True),
        lax.all_gather(w_value, "sp", axis=0, tiled=True),
    )
    key_rows = jnp.dot(token_rows, whole_key, preferred_element_type=jnp.float32).astype(
        jnp.bfloat16
    )
    value_rows = jnp.dot(token_rows, whole_value, preferred_element_type=jnp.float32).astype(
        jnp.bfloat16
    )
    head_start = lax.axis_index("tp") * local_heads
    input_all = jnp.dot(token_rows, w_igate, preferred_element_type=jnp.float32) + input_bias
    forget_all = jnp.dot(token_rows, w_fgate, preferred_element_type=jnp.float32) + forget_bias
    input_gate = lax.dynamic_slice_in_dim(input_all, head_start, local_heads, 1).reshape(
        seq_count, span_len, local_heads
    )
    log_forget = jax.nn.log_sigmoid(
        lax.dynamic_slice_in_dim(forget_all, head_start, local_heads, 1)
    ).reshape(seq_count, span_len, local_heads)
    block_total = jnp.sum(log_forget, axis=1)
    forget_after = block_total[:, None] - jnp.cumsum(log_forget, axis=1)
    log_weight = forget_after + input_gate
    block_max = jnp.max(log_weight, axis=1)
    key_blocks = key_rows.reshape(seq_count, span_len, local_heads, key_size).astype(jnp.float32)
    decayed = (jnp.exp(log_weight - block_max[:, None])[..., None] * key_scale * key_blocks).astype(
        jnp.bfloat16
    )
    value_blocks = value_rows.reshape(seq_count, span_len, local_heads, value_size)
    block_norm = jnp.sum(decayed.astype(jnp.float32), axis=1)
    later_total = entering(block_total, "sp", add_pair, jnp.zeros_like(block_total))
    block_lift = later_total + block_max
    global_max = lax.pmax(block_lift, "sp")
    factor = jnp.exp(block_lift - global_max)
    scaled_norm = factor[:, :, None] * block_norm
    query_full = new_query.astype(jnp.float32)
    block_state = jnp.einsum(
        "sthk,sthv->shkv", decayed, value_blocks, preferred_element_type=jnp.float32
    )
    scaled_state = factor[:, :, None, None] * block_state
    memory_rows, norm_rows = (
        lax.psum_scatter(scaled_state, "sp", scatter_dimension=2, tiled=True),
        lax.psum_scatter(scaled_norm, "sp", scatter_dimension=2, tiled=True),
    )
    token_score = jnp.einsum(
        "shk,sthk->sth", new_query, decayed, preferred_element_type=jnp.float32
    )
    score_high = token_score.astype(jnp.bfloat16)
    score_low = (token_score - score_high.astype(jnp.float32)).astype(jnp.bfloat16)
    weighted = jnp.einsum(
        "sth,sthv->shv", score_high, value_blocks, preferred_element_type=jnp.float32
    )
    weighted = weighted + jnp.einsum(
        "sth,sthv->shv", score_low, value_blocks, preferred_element_type=jnp.float32
    )
    partial_state = factor[..., None] * weighted
    partial_norm = jnp.sum(query_full * scaled_norm, axis=-1)
    query_state, query_norm = lax.psum((partial_state, partial_norm), "sp")
    forget_new = jax.nn.log_sigmoid(new_gates[1])
    input_new = new_gates[0]
    mixed = jnp.maximum(forget_new + global_max, input_new)
    carried = jnp.exp(forget_new + global_max - mixed)
    fresh = jnp.exp(input_new - mixed)
    own_score = jnp.sum(query_full * new_key.astype(jnp.float32), axis=-1) * key_scale
    numer = carried[..., None] * query_state + (fresh * own_score)[..., None] * new_value.astype(
        jnp.float32
    )
    denom = carried * query_norm + fresh * own_score
    first_read = (numer / jnp.maximum(jnp.abs(denom), 1.0)[..., None]).astype(jnp.bfloat16)
    return (memory_rows.astype(jnp.bfloat16), norm_rows, global_max, first_read)


def solution(mesh):
    placed = (
        P(None, "sp", None),
        P("sp", "tp"),
        P("sp", "tp"),
        P(),
        P(),
        P(),
        P(),
        P(None, "tp", None),
        P(None, "tp", None),
        P(None, "tp", None),
        P(None, None, "tp"),
    )
    return jax.shard_map(
        chosen,
        mesh=mesh,
        in_specs=placed,
        out_specs=(
            P(None, "tp", "sp", None),
            P(None, "tp", "sp"),
            P(None, "tp"),
            P(None, "tp", None),
        ),
        check_vma=False,
    )
```
